512 devices in a mesh: sp: 32 (over z, core), tp: 16 (over y, x).
Axes of the slice: x: 4, y: 4, z: 16, core: 2. Of those that a mesh axis runs over, the one named last changes fastest.
Arguments:
- residual: bfloat16 [4096, 2048], P('sp', 'tp'), may hold values from -48 to 48
- glu_value: bfloat16 [4096, 2048], P('sp', 'tp'), may hold values from -48 to 48
- glu_gate: bfloat16 [4096, 2048], P('sp', 'tp'), may hold values from -6 to 6
- conv_weight: bfloat16 [31, 2048], P(None, 'tp'), may hold values from -1 to 1
- conv_bias: float32 [2048], P('tp'), may hold values from -3 to 3
- ln_gain: float32 [2048], P('tp'), may hold values from 0.1 to 1.9
- ln_bias: float32 [2048], P('tp'), may hold values from -3 to 3
- out_weight: bfloat16 [2048, 2048], P(None, 'tp'), may hold values from -0.125 to 0.125
- norm_gain: float32 [2048], P('tp'), may hold values from 0.1 to 1.9
- route_ids: int32 [4096, 2], P('sp'), may hold values from 0 to 31, all different within a row; in each aligned block of 128 rows (0 to 127, 128 to 255, ...) at most 16 rows name the same one
- route_weight: float32 [4096, 2], P('sp'), may hold values from 0.1 to 1
- expert_gate: bfloat16 [32, 2048, 4096], P('sp', None, 'tp'), may hold values from -0.125 to 0.125
- expert_up: bfloat16 [32, 2048, 4096], P('sp', None, 'tp'), may hold values from -0.125 to 0.125
- expert_down: bfloat16 [32, 4096, 2048], P('sp', 'tp'), may hold values from -0.09375 to 0.09375
Outputs:
- layer_out: bfloat16 [4096, 2048], P('sp', 'tp')
The draws below stay inside these ranges and needn't reach their ends.
Inputs may be any that keep to these rules, and one draw needn't show every extreme that they name: `route_ids`: within the 128 rows of one index of sp, no expert is named more than 16 times, and in some such rows one expert is named exactly 16 times.
All inputs are finite; a program needn't handle non-finite values.
Results may differ from the reference program's by a relative error of at most 0.006.
Values may be sent and summed in bfloat16 or wider, within the bound.
A program may use at most 64 MiB of HBM per device.

```python
import math
import jax
import jax.numpy as jnp
import numpy as np
from jax import lax

D = 2048
FF = 4096
KERNEL = 31
TOPK = 2
ROWS = 128
TOKENS = 4096
EXPERTS = 32
CAP = 16
N_SP = 32
N_TP = 16


def rising_field(key, low, high):
    ramp = jnp.exp(jnp.linspace(math.log(low), math.log(high), D)).astype(jnp.float32)
    base = jnp.clip(jax.random.normal(key, (TOKENS, D), jnp.float32), -6.0, 6.0)
    return base * ramp


def draw_residual(key, part):
    return rising_field(jax.random.fold_in(key, 11), 0.5, 2.0).astype(jnp.bfloat16)


def draw_glu_value(key, part):
    return rising_field(jax.random.fold_in(key, 23), 0.5, 2.0).astype(jnp.bfloat16)


def levels(stream_key, dims, shards, least, largest):
    def one(position, parts):
        heights = jax.random.uniform(jax.random.fold_in(jax.random.fold_in(stream_key, 6), position), (parts,), jnp.float32, least / len(shards), largest / len(shards))
        return jnp.repeat(jnp.exp(heights), dims[position] // parts).reshape((-1,) + (1,) * (len(dims) - position - 1))

    loudness = one(*shards[0])
    for cut in shards[1:]:
        loudness = loudness * one(*cut)
    return loudness


def routed_block(rng, own, number, rows, count, top, most, skew):
    order = jax.random.permutation(rng, count)
    heavy_load, ordinary = portions_of(count, rows * top, most, skew, True), portions_of(count, rows * top, most, skew, False)
    places = jnp.arange(count)

    def named(lengths, turn):
        used = int((lengths > 0).sum())
        fixed = max(1, used // 4)
        moved = fixed + (places - fixed + turn * (used - fixed)) % max(1, count - fixed)
        return jnp.zeros((count,), jnp.int32).at[order[jnp.where(places < fixed, places, moved)]].set(jnp.asarray(lengths, jnp.int32))

    lengths = jnp.where(number % 4 == 0, named(heavy_load, number // 4), named(ordinary, number - number // 4 - 1))
    mixed = jax.random.permutation(jax.random.fold_in(own, 3), count)
    giver, sink = mixed[0:count // 2 * 2:2], mixed[1:count // 2 * 2:2]
    slack = jnp.minimum(lengths[giver] - 1, most - lengths[sink]) // 2
    slack = jnp.where((giver == order[0]) | (sink == order[0]) | (lengths[sink] == 0), 0, jnp.maximum(slack, 0))
    moved = jax.random.randint(jax.random.fold_in(own, 4), (count // 2,), 0, 1 << 20) % (slack + 1)
    lengths = lengths.at[giver].add(-moved).at[sink].add(moved)
    items = jnp.searchsorted(jnp.cumsum(lengths), jnp.arange(rows * top), side="right").astype(jnp.int32)
    table = items.reshape(top, rows).T
    table = table[jax.random.permutation(jax.random.fold_in(own, 1), rows)]
    turn = jax.random.randint(jax.random.fold_in(own, 2), (rows, 1), 0, top)
    return jnp.take_along_axis(table, (jnp.arange(top)[None, :] + turn) % top, axis=1)


def portions_of(count, total, bound, lean, full):
    loads = [(1 << 20) // math.isqrt(rank ** lean) + 1 for rank in range(1, count + 1)]
    largest = bound if full else min(bound, max(-(-total // count), total * loads[0] // sum(loads)))
    least = 1 if total - largest >= count - 1 else 0
    counts, spare = [largest] + [least] * (count - 1), total - largest - least * (count - 1)
    while spare > 0:
        candidates = [i for i in range(1, count) if counts[i] < largest] or [i for i in range(1, count) if counts[i] < bound]
        whole, left = sum([loads[i] for i in candidates]), spare
        for i in candidates:
            extra = min(bound - counts[i], max(1, left * loads[i] // whole), spare)
            counts[i] = counts[i] + extra
            spare = spare - extra
    return np.array(counts)


def gaussian(rng, shape, spread, limit, cuts=(), kind=jnp.bfloat16):
    drawn = spread * jax.random.normal(rng, shape, jnp.float32)
    if cuts:
        drawn = drawn * levels(rng, shape, cuts, -0.22, 0.18)
    return jnp.clip(drawn, -limit, limit).astype(kind)


def setup_inputs(seed: int = 0) -> dict:
    arg_keys = jax.random.split(jax.random.key(seed), 15)
    residual = draw_residual(jax.random.fold_in(arg_keys[14], 71), 0)
    glu_value = draw_glu_value(jax.random.fold_in(arg_keys[14], 71), 0)
    glu_gate = gaussian(arg_keys[2], (TOKENS, D), 1.0, 6.0, ((0, 32), (1, 16)))
    conv_weight = gaussian(arg_keys[3], (KERNEL, D), KERNEL ** -0.5, 1.0, ((1, 16),))
    conv_bias = gaussian(arg_keys[4], (D,), 0.5, 3.0, ((0, 16),), jnp.float32)
    ln_gain = jnp.clip(1.0 + 0.18 * jax.random.normal(arg_keys[5], (D,), jnp.float32), 0.1, 1.9)
    ln_bias = gaussian(arg_keys[6], (D,), 0.5, 3.0, ((0, 16),), jnp.float32)
    out_weight = gaussian(arg_keys[7], (D, D), D ** -0.5, 0.125, ((1, 16),))
    norm_gain = jnp.clip(1.0 + 0.18 * jax.random.normal(arg_keys[8], (D,), jnp.float32), 0.1, 1.9)
    route_ids_keys = jax.random.split(jax.random.fold_in(arg_keys[9], 1), TOKENS // ROWS)
    route_ids_turns = jax.random.permutation(jax.random.fold_in(arg_keys[9], 3), TOKENS // ROWS)
    route_ids = jax.vmap(lambda own, number: routed_block(jax.random.fold_in(arg_keys[9], 2), own, number, ROWS, EXPERTS, TOPK, CAP, 2))(route_ids_keys, route_ids_turns).reshape((TOKENS, TOPK))
    route_weight = jnp.clip(jnp.exp(math.log(1.0) - 2.3025851 * jax.random.uniform(arg_keys[10], (TOKENS, TOPK), jnp.float32) ** levels(arg_keys[10], (TOKENS, TOPK), ((0, 32),), -0.2, 0.2)), 0.1, 1.0)
    expert_gate = gaussian(arg_keys[11], (EXPERTS, D, FF), D ** -0.5, 0.125, ((0, 32), (2, 16)))
    expert_up = gaussian(arg_keys[12], (EXPERTS, D, FF), D ** -0.5, 0.125, ((0, 32), (2, 16)))
    expert_down = gaussian(arg_keys[13], (EXPERTS, FF, D), FF ** -0.5, 0.09375, ((0, 32), (1, 16)))
    return dict(residual=residual, glu_value=glu_value, glu_gate=glu_gate, conv_weight=conv_weight, conv_bias=conv_bias, ln_gain=ln_gain, ln_bias=ln_bias, out_weight=out_weight, norm_gain=norm_gain, route_ids=route_ids, route_weight=route_weight, expert_gate=expert_gate, expert_up=expert_up, expert_down=expert_down)


def reference(residual, glu_value, glu_gate, conv_weight, conv_bias, ln_gain, ln_bias, out_weight, norm_gain, route_ids, route_weight, expert_gate, expert_up, expert_down):
    gated = (glu_value.astype(jnp.float32) * jax.nn.sigmoid(glu_gate.astype(jnp.float32))).astype(jnp.bfloat16)
    reach = KERNEL // 2
    padded = jnp.pad(gated.astype(jnp.float32), ((reach, reach), (0, 0)))
    taps = conv_weight.astype(jnp.float32)
    conv = jnp.zeros(gated.shape, jnp.float32) + conv_bias
    for tap in range(KERNEL):
        conv = conv + padded[tap:tap + TOKENS] * taps[tap]
    mean = lax.optimization_barrier(jnp.mean(conv, axis=1, keepdims=True))
    var = lax.optimization_barrier(jnp.mean(conv * conv, axis=1, keepdims=True)) - mean * mean
    act = jax.nn.silu((conv - mean) * lax.rsqrt(var + 1e-05) * ln_gain + ln_bias).astype(jnp.bfloat16)
    mixed = residual.astype(jnp.float32) + jnp.dot(act, out_weight, preferred_element_type=jnp.float32)
    squares = lax.optimization_barrier(jnp.mean(mixed * mixed, axis=1, keepdims=True))
    normed = (mixed * lax.rsqrt(squares + 1e-06) * norm_gain).astype(jnp.bfloat16)
    flat = route_ids.reshape(-1)
    owner = (jnp.arange(TOKENS * TOPK, dtype=jnp.int32) // TOPK).astype(jnp.int32)
    weights = route_weight.reshape(-1)
    slots = N_SP * CAP
    slot_index = jnp.arange(slots, dtype=jnp.int32)
    block = FF // N_TP

    def per_expert(total, expert):
        chosen = flat == expert
        picks = jnp.nonzero(chosen, size=slots, fill_value=0)[0].astype(jnp.int32)
        count = jnp.sum(chosen.astype(jnp.int32))
        live = (slot_index < count).astype(jnp.float32)
        rows = normed[owner[picks]]
        gate = jnp.dot(rows, expert_gate[expert], preferred_element_type=jnp.float32)
        up = jnp.dot(rows, expert_up[expert], preferred_element_type=jnp.float32)
        hidden = (jax.nn.silu(gate) * up).astype(jnp.bfloat16)
        down = expert_down[expert]
        result = jnp.zeros((slots, D), jnp.float32)
        for part_index in range(N_TP):
            piece = jnp.dot(hidden[:, part_index * block:(part_index + 1) * block], down[part_index * block:(part_index + 1) * block], preferred_element_type=jnp.float32)
            result = result + piece.astype(jnp.bfloat16).astype(jnp.float32)
        result = result.astype(jnp.bfloat16)
        scaled = result.astype(jnp.float32) * (weights[picks] * live)[:, None]
        return (total.at[owner[picks]].add(scaled), None)
    moe, _ = lax.scan(per_expert, jnp.zeros((TOKENS, D), jnp.float32), jnp.arange(EXPERTS, dtype=jnp.int32))
    return (mixed + moe).astype(jnp.bfloat16)
```

```python
import functools

import jax
import jax.numpy as jnp
from jax import lax
from jax.experimental import pallas as pl
from jax.experimental.pallas import tpu as pltpu
from jax.sharding import PartitionSpec as P

MESH = pl.DeviceIdType.MESH
TOPK = 2
F32 = jnp.float32
BF16 = jnp.bfloat16
NX = 4
CHUNKS = 2

TREE_4X4 = {
    (1, 0): (0, 0),
    (3, 0): (0, 0),
    (0, 1): (0, 0),
    (0, 3): (0, 0),
    (1, 1): (1, 0),
    (3, 1): (0, 1),
    (3, 3): (3, 0),
    (1, 3): (0, 3),
    (2, 0): (1, 0),
    (0, 2): (0, 3),
    (2, 1): (3, 1),
    (2, 3): (1, 3),
    (1, 2): (1, 1),
    (3, 2): (3, 3),
    (2, 2): (2, 1),
}


def spanning_tree(nx, ny):
    if (nx, ny) == (4, 4):
        parent = TREE_4X4
    else:
        parent, frontier = {}, [(0, 0)]
        while frontier:
            grown = []
            for px, py in frontier:
                for dx, dy in ((1, 0), (nx - 1, 0), (0, 1), (0, ny - 1)):
                    o = ((px + dx) % nx, (py + dy) % ny)
                    if o != (0, 0) and o not in parent:
                        parent[o] = (px, py)
                        grown.append(o)
            frontier = grown
    depth = {(0, 0): 0}
    order = [(0, 0)]
    for o in order:
        for c, p in parent.items():
            if p == o:
                depth[c] = depth[o] + 1
                order.append(c)
    order.sort(key=lambda o: depth[o])
    children = {o: [c for c in order if parent.get(c) == o] for o in order}
    height = {}
    for o in reversed(order):
        height[o] = 1 + max([height[c] for c in children[o]], default=-1)
    return order, parent, children, depth, height


def layer_kernel(
    ns,
    nx,
    ny,
    residual_ref,
    value_ref,
    gate_ref,
    taps_ref,
    conv_bias_ref,
    ln_gain_ref,
    ln_bias_ref,
    out_weight_hbm,
    norm_gain_ref,
    ids_ref,
    route_weight_ref,
    expert_gate_hbm,
    expert_up_hbm,
    expert_down_hbm,
    out_ref,
    out_weight,
    expert_gate,
    expert_up,
    expert_down,
    halo,
    gated,
    padded,
    stat,
    act,
    mixed,
    picks,
    places,
    outgoing,
    xbuf,
    acc_gate,
    acc_up,
    acc_sq,
    partial,
    rs_in,
    rs_out,
    ret_out,
    ret_in,
    weight_sem,
    halo_s,
    halo_r,
    stat_s,
    stat_r,
    act_s,
    act_r,
    z_s,
    z_r,
    ag_s,
    ag_r,
    rs_s,
    rs_r,
    rt_s,
    rt_r,
):
    ntp = nx * ny
    rows, width = residual_ref.shape
    total_width = ntp * width
    slots = places.shape[0]
    cap = slots // ns
    chunks = outgoing.shape[0]
    depth_rows = slots // chunks
    per_side = ns // (2 * chunks)
    taps = taps_ref.shape[0]
    reach = taps // 2
    edge = halo.shape[1]
    s = lax.axis_index("sp")
    t = lax.axis_index("tp")
    ty, tx = t // nx, lax.rem(t, nx)
    order, parent, children, depth, height = spanning_tree(nx, ny)
    number = {o: i for i, o in enumerate(order)}

    def tp_at(dx, dy):
        return lax.rem(ty + dy + 2 * ny, ny) * nx + lax.rem(tx + dx + 2 * nx, nx)

    def owner(o):
        return tp_at(-o[0], -o[1])

    def sp_at(d):
        return lax.rem(s + d + 2 * ns, ns)

    def distance(k, jj):
        return k * per_side + jj if jj < per_side else jj - (k + 2) * per_side

    def send(src, dst, send_sem, recv_sem, device):
        copy = pltpu.make_async_remote_copy(
            src_ref=src,
            dst_ref=dst,
            send_sem=send_sem,
            recv_sem=recv_sem,
            device_id=device,
            device_id_type=MESH,
        )
        copy.start()
        return copy

    barrier = pltpu.get_barrier_semaphore()
    for i in range(1, ntp):
        pl.semaphore_signal(
            barrier, inc=1, device_id=(s, lax.rem(t + i, ntp)), device_id_type=MESH
        )
    for d in range(1, ns):
        pl.semaphore_signal(barrier, inc=1, device_id=(sp_at(d), t), device_id_type=MESH)

    loads = [
        pltpu.make_async_copy(out_weight_hbm, out_weight, weight_sem.at[0]),
        pltpu.make_async_copy(expert_gate_hbm.at[0], expert_gate, weight_sem.at[1]),
        pltpu.make_async_copy(expert_up_hbm.at[0], expert_up, weight_sem.at[2]),
        pltpu.make_async_copy(expert_down_hbm.at[0], expert_down, weight_sem.at[3]),
    ]
    for load in loads:
        load.start()

    gated_f = value_ref[...].astype(F32) * jax.nn.sigmoid(gate_ref[...].astype(F32))
    gated[...] = gated_f.astype(BF16)
    padded[edge : edge + rows, :] = gated[...].astype(F32)

    expert_of = lax.broadcasted_iota(jnp.int32, (rows, ns), 1)
    chosen = [
        jnp.where(ids_ref[:, k : k + 1] == expert_of, 1.0, 0.0).astype(BF16)
        for k in range(TOPK)
    ]
    earlier = jnp.where(
        lax.broadcasted_iota(jnp.int32, (rows, rows), 1)
        < lax.broadcasted_iota(jnp.int32, (rows, rows), 0),
        1.0,
        0.0,
    ).astype(BF16)
    rank = jnp.dot(earlier, chosen[0] + chosen[1], preferred_element_type=F32).astype(BF16)
    slot = lax.broadcasted_iota(jnp.int32, (ns, slots), 1)
    in_chunk = (slot // cap) & (2 * per_side - 1)
    chunk_of = slot // depth_rows
    away = in_chunk + chunk_of * per_side
    away = jnp.where(in_chunk >= per_side, away - (2 * chunk_of + 2) * per_side, away)
    spread = jnp.where(
        lax.broadcasted_iota(jnp.int32, (ns, slots), 0) == ((s + away + 2 * ns) & (ns - 1)),
        1.0,
        0.0,
    ).astype(BF16)
    rank_at = jnp.dot(rank, spread, preferred_element_type=F32)
    slot_rank = (lax.broadcasted_iota(jnp.int32, (rows, slots), 1) & (cap - 1)).astype(F32)
    hit = rank_at == slot_rank
    both = jnp.zeros((rows, slots), F32)
    for k in range(TOPK):
        here = jnp.dot(chosen[k], spread, preferred_element_type=F32)
        here = jnp.where(hit, here, 0.0)
        picks[k] = here.astype(BF16)
        both = both + here
    places[...] = both.T.astype(BF16)

    ln_gain_col = jnp.broadcast_to(ln_gain_ref[...], (rows, width)).T
    ln_bias_col = jnp.broadcast_to(ln_bias_ref[...], (rows, width)).T

    pl.semaphore_wait(barrier, ntp - 1 + ns - 1)

    to_right = send(
        gated.at[pl.ds(rows - edge, edge)], halo.at[0], halo_s.at[0], halo_r.at[0], (sp_at(1), t)
    )
    to_left = send(gated.at[pl.ds(0, edge)], halo.at[1], halo_s.at[1], halo_r.at[1], (sp_at(-1), t))
    pending = [to_right, to_left]
    to_right.wait_recv()
    to_left.wait_recv()
    padded[0:edge, :] = jnp.where(s > 0, halo[0].astype(F32), 0.0)
    padded[edge + rows : edge + rows + edge, :] = jnp.where(
        s < ns - 1, halo[1].astype(F32), 0.0
    )
    tap_values = taps_ref[...].astype(F32)
    conv = jnp.zeros((rows, width), F32) + conv_bias_ref[...]
    for tap in range(taps):
        start = edge - reach + tap
        conv = conv + padded[start : start + rows, :] * tap_values[tap : tap + 1, :]
    conv_t = conv.T
    stat_row = jnp.concatenate(
        [
            jnp.sum(conv_t, axis=0, keepdims=True),
            jnp.sum(conv_t * conv_t, axis=0, keepdims=True),
            1.0 / norm_gain_ref[...],
            jnp.zeros((5, width), F32),
        ],
        axis=0,
    )
    stat[t] = stat_row
    arriving = []
    for i in range(1, ntp):
        arriving.append(
            send(
                stat.at[t],
                stat.at[t],
                stat_s.at[i],
                stat_r.at[i],
                (s, lax.rem(t + i, ntp)),
            )
        )
    for copy in arriving:
        copy.wait_recv()
    pending += arriving
    totals = jnp.sum(stat[...], axis=0) * (1.0 / total_width)
    mean = totals[0:1, :]
    var = totals[1:2, :] - mean * mean
    scaled = (conv_t - mean) * lax.rsqrt(var + 1e-05) * ln_gain_col + ln_bias_col
    act[t] = jax.nn.silu(scaled).T.astype(BF16)
    arriving = []
    for i in range(1, ntp):
        arriving.append(
            send(act.at[t], act.at[t], act_s.at[i], act_r.at[i], (s, lax.rem(t + i, ntp)))
        )
    loads[0].wait()
    for copy in arriving:
        copy.wait_recv()
    pending += arriving
    all_act = jnp.concatenate([act[i] for i in range(ntp)], axis=1)
    projected = jnp.dot(all_act, out_weight[...], preferred_element_type=F32)
    total = residual_ref[...].astype(F32) + projected
    mixed[...] = total
    scaled_rows = (total * norm_gain_ref[...]).astype(BF16)

    dispatch = {}
    for k in range(chunks):
        outgoing[k] = jnp.dot(
            places[k * depth_rows : (k + 1) * depth_rows, :],
            scaled_rows,
            preferred_element_type=F32,
        ).astype(BF16)
        for jj in range(2 * per_side):
            d = distance(k, jj)
            part = pl.ds(jj * cap, cap)
            if d == 0:
                xbuf[k, 0, part, :] = outgoing[k, part, :]
            else:
                dispatch[k, jj] = send(
                    outgoing.at[k, part],
                    xbuf.at[k, 0, part],
                    z_s.at[k, jj],
                    z_r.at[k, jj],
                    (sp_at(d), t),
                )
    pending += list(dispatch.values())
    for load in loads[1:]:
        load.wait()

    gathers, sums, returns = {}, {}, {}

    def pass_on(k, o):
        if o == (0, 0):
            for (kk, _), copy in dispatch.items():
                if kk == k:
                    copy.wait_recv()
        else:
            gathers[k, o].wait_recv()
        for c in children[o]:
            gathers[k, c] = send(
                xbuf.at[k, number[o]],
                xbuf.at[k, number[c]],
                ag_s.at[k, number[c]],
                ag_r.at[k, number[c]],
                (s, tp_at(c[0] - o[0], c[1] - o[1])),
            )

    def multiply(k, group, first):
        blocks = [xbuf[k, number[o]] for o in group]
        owners = [owner(o) for o in group]
        wide = jnp.concatenate(blocks, axis=1)
        squares = None if first else acc_sq[k]
        for block, who in zip(blocks, owners):
            plain = block.astype(F32) * stat[who, 2:3, :]
            squares = plain * plain if squares is None else squares + plain * plain
        acc_sq[k] = squares
        for weight, acc in ((expert_gate, acc_gate), (expert_up, acc_up)):
            tall = jnp.concatenate(
                [weight[pl.ds(pl.multiple_of(who * width, width), width), :] for who in owners],
                axis=0,
            )
            product = jnp.dot(wide, tall, preferred_element_type=F32)
            acc[k] = product if first else acc[k] + product

    def finish_rows(k):
        square = jnp.sum(acc_sq[k], axis=1, keepdims=True) * (1.0 / total_width)
        scale = lax.rsqrt(square + 1e-06)
        hidden = (jax.nn.silu(acc_gate[k] * scale) * (acc_up[k] * scale)).astype(BF16)
        for i in range(ntp):
            partial[k, i] = jnp.dot(
                hidden, expert_down[:, i * width : (i + 1) * width], preferred_element_type=F32
            ).astype(BF16)

    def sum_up(k, o):
        who = owner(o)
        source = partial.at[k, who]
        if children[o]:
            value = partial[k, who].astype(F32)
            for c in children[o]:
                sums[k, c].wait_recv()
                value = value + rs_in[k, number[c]].astype(F32)
            if o == (0, 0):
                ret_out[k] = value.astype(BF16)
                return
            rs_out[k, number[o]] = value.astype(BF16)
            source = rs_out.at[k, number[o]]
        p = parent[o]
        sums[k, o] = send(
            source,
            rs_in.at[k, number[o]],
            rs_s.at[k, number[o]],
            rs_r.at[k, number[o]],
            (s, tp_at(p[0] - o[0], p[1] - o[1])),
        )

    def give_back(k):
        for jj in range(2 * per_side):
            d = distance(k, jj)
            part = pl.ds(jj * cap, cap)
            if d == 0:
                ret_in[k, part, :] = ret_out[k, part, :]
            else:
                returns[k, jj] = send(
                    ret_out.at[k, part],
                    ret_in.at[k, part],
                    rt_s.at[k, jj],
                    rt_r.at[k, jj],
                    (sp_at(-d), t),
                )

    levels = max(depth.values())
    heights = max(height.values())
    split = max(1, levels // 2)
    events = []
    for k in range(chunks):
        base = 2.0 * k
        for level in range(levels + 1):
            at = [o for o in order if depth[o] == level]
            events.append((base + level, [functools.partial(pass_on, k, o) for o in at]))
        groups = [
            [o for o in order if depth[o] <= 1],
            [o for o in order if depth[o] == 2],
            [o for o in order if depth[o] > 2],
        ]
        for i, group in enumerate(groups):
            if group:
                when = base + max(depth[o] for o in group) + 0.5
                events.append((when, [functools.partial(multiply, k, group, i == 0)]))
        events.append((base + levels + 0.6, [functools.partial(finish_rows, k)]))
        for h in range(heights + 1):
            at = [o for o in order if height[o] == h]
            at.sort(key=lambda o: -depth[o])
            events.append(
                (base + levels + 0.7 + 1.2 * h, [functools.partial(sum_up, k, o) for o in at])
            )
        events.append(
            (base + levels + 0.8 + 1.2 * heights, [functools.partial(give_back, k)])
        )
    events.sort(key=lambda e: e[0])
    for _, steps in events:
        for step in steps:
            step()

    for copy in returns.values():
        copy.wait_recv()
    answer = jnp.concatenate([ret_in[k] for k in range(chunks)], axis=0)
    result = mixed[...]
    for k in range(TOPK):
        picked = jnp.dot(picks[k], answer, preferred_element_type=F32)
        result = result + picked * route_weight_ref[:, k : k + 1]
    out_ref[...] = result.astype(BF16)

    pending += list(gathers.values()) + list(sums.values()) + list(returns.values())
    for copy in pending:
        copy.wait_send()


def on_device(ns, nx, ny, *args):
    (
        residual,
        glu_value,
        glu_gate,
        conv_weight,
        conv_bias,
        ln_gain,
        ln_bias,
        out_weight,
        norm_gain,
        route_ids,
        route_weight,
        expert_gate,
        expert_up,
        expert_down,
    ) = args
    ntp = nx * ny
    rows, width = residual.shape
    hidden = expert_gate.shape[2]
    capacity = 2 * rows * TOPK // ns
    slots = ns * capacity
    k, rc = CHUNKS, slots // CHUNKS
    edge = 16
    row = lambda v: v.reshape(1, -1)
    vmem = pl.BlockSpec(memory_space=pltpu.VMEM)
    hbm = pl.BlockSpec(memory_space=pltpu.HBM)
    dma = pltpu.SemaphoreType.DMA
    return pl.pallas_call(
        functools.partial(layer_kernel, ns, nx, ny),
        out_shape=jax.ShapeDtypeStruct(residual.shape, BF16),
        in_specs=[vmem] * 7 + [hbm] + [vmem] * 3 + [hbm] * 3,
        out_specs=vmem,
        scratch_shapes=[
            pltpu.VMEM(out_weight.shape, BF16),
            pltpu.VMEM(expert_gate.shape[1:], BF16),
            pltpu.VMEM(expert_up.shape[1:], BF16),
            pltpu.VMEM(expert_down.shape[1:], BF16),
            pltpu.VMEM((2, edge, width), BF16),
            pltpu.VMEM((rows, width), BF16),
            pltpu.VMEM((rows + 2 * edge, width), F32),
            pltpu.VMEM((ntp, 8, width), F32),
            pltpu.VMEM((ntp, rows, width), BF16),
            pltpu.VMEM((rows, width), F32),
            pltpu.VMEM((TOPK, rows, slots), BF16),
            pltpu.VMEM((slots, rows), BF16),
            pltpu.VMEM((k, rc, width), BF16),
            pltpu.VMEM((k, ntp, rc, width), BF16),
            pltpu.VMEM((k, rc, hidden), F32),
            pltpu.VMEM((k, rc, hidden), F32),
            pltpu.VMEM((k, rc, width), F32),
            pltpu.VMEM((k, ntp, rc, width), BF16),
            pltpu.VMEM((k, ntp, rc, width), BF16),
            pltpu.VMEM((k, ntp, rc, width), BF16),
            pltpu.VMEM((k, rc, width), BF16),
            pltpu.VMEM((k, rc, width), BF16),
            dma((4,)),
            dma((2,)),
            dma((2,)),
            dma((ntp,)),
            dma((ntp,)),
            dma((ntp,)),
            dma((ntp,)),
            dma((k, ns // k)),
            dma((k, ns // k)),
            dma((k, ntp)),
            dma((k, ntp)),
            dma((k, ntp)),
            dma((k, ntp)),
            dma((k, ns // k)),
            dma((k, ns // k)),
        ],
        compiler_params=pltpu.CompilerParams(
            collective_id=0, has_side_effects=True, vmem_limit_bytes=48 * 1024 * 1024
        ),
        name="layer",
    )(
        residual,
        glu_value,
        glu_gate,
        conv_weight,
        row(conv_bias),
        row(ln_gain),
        row(ln_bias),
        out_weight,
        row(norm_gain),
        route_ids,
        route_weight,
        expert_gate,
        expert_up,
        expert_down,
    )


IN_SPECS = (
    P("sp", "tp"),
    P("sp", "tp"),
    P("sp", "tp"),
    P(None, "tp"),
    P("tp"),
    P("tp"),
    P("tp"),
    P(None, "tp"),
    P("tp"),
    P("sp", None),
    P("sp", None),
    P("sp", None, "tp"),
    P("sp", None, "tp"),
    P("sp", "tp", None),
)


def solution(mesh, nx=NX):
    ns, ntp = mesh.shape["sp"], mesh.shape["tp"]
    return jax.shard_map(
        functools.partial(on_device, ns, nx, ntp // nx),
        mesh=mesh,
        in_specs=IN_SPECS,
        out_specs=P("sp", "tp"),
        check_vma=False,
    )
```

```python
import functools

import jax
import jax.numpy as jnp
from jax import lax
from jax.experimental import pallas as pl
from jax.experimental.pallas import tpu as pltpu
from jax.sharding import PartitionSpec as P

MESH = pl.DeviceIdType.MESH
TOPK = 2
F32 = jnp.float32
BF16 = jnp.bfloat16
NX = 4
CHUNKS = 4
SEND_ORDER = (0, 2, 3, 1)
URGENCY = (1, 0, 2, 3)
KINDS = (0, 0, 0, 1)

TREE_4X4 = {
    (1, 0): (0, 0),
    (3, 0): (0, 0),
    (0, 1): (0, 0),
    (0, 3): (0, 0),
    (1, 1): (1, 0),
    (3, 1): (0, 1),
    (3, 3): (3, 0),
    (1, 3): (0, 3),
    (2, 0): (1, 0),
    (0, 2): (0, 3),
    (2, 1): (3, 1),
    (2, 3): (1, 3),
    (1, 2): (1, 1),
    (3, 2): (3, 3),
    (2, 2): (2, 1),
}
SHALLOW_4X4 = {
    **{o: (0, 0) for o in TREE_4X4},
    (2, 0): (1, 0),
    (0, 2): (0, 3),
    (2, 1): (1, 1),
    (2, 3): (3, 3),
    (1, 2): (1, 3),
    (3, 2): (3, 1),
    (2, 2): (1, 1),
}


def turned(tree, quarters):
    def turn(o):
        for _ in range(quarters):
            o = (-o[1] % 4, o[0])
        return o

    return {turn(c): turn(p) for c, p in tree.items()}


class Tree:
    def __init__(self, nx, ny, kind, quarters):
        if (nx, ny) == (4, 4):
            parent = turned(SHALLOW_4X4 if kind else TREE_4X4, quarters)
        else:
            parent, frontier = {}, [(0, 0)]
            while frontier:
                grown = []
                for px, py in frontier:
                    for dx, dy in ((1, 0), (nx - 1, 0), (0, 1), (0, ny - 1)):
                        o = ((px + dx) % nx, (py + dy) % ny)
                        if o != (0, 0) and o not in parent:
                            parent[o] = (px, py)
                            grown.append(o)
                frontier = grown
        self.parent = parent
        self.depth = {(0, 0): 0}
        self.order = [(0, 0)]
        for o in self.order:
            for c in sorted(parent):
                if parent[c] == o:
                    self.depth[c] = self.depth[o] + 1
                    self.order.append(c)
        self.children = {o: [c for c in self.order if parent.get(c) == o] for o in self.order}
        self.groups = [
            [o for o in self.order if low <= self.depth[o] <= high]
            for low, high in ((0, 1), (2, 2), (3, 9))
        ]
        self.groups = [g for g in self.groups if g]


def signed(v, n):
    return (v + n // 2 - 1) % n - (n // 2 - 1)


def plan(trees, nx, ny, rows, arrivals, urgency):
    wire, latency, hop = rows * 256 / 46.65e3, 2.2, 0.75
    link, now, steps, pending = {}, 0.0, [], []
    arrived, summed, passed, given = {}, {}, {}, {}

    def sent(p, o):
        dx, dy = signed(o[0] - p[0], nx), signed(o[1] - p[1], ny)
        end = now
        for axis, v, n in ((0, dx, nx), (1, dy, ny)):
            if v:
                for way in (1, -1) if 2 * v == n else (1 if v > 0 else -1,):
                    link[axis, way] = max(link.get((axis, way), 0.0), now) + wire
                    end = max(end, link[axis, way])
        return end + latency + hop * (abs(dx) + abs(dy) - 1)

    for k in range(len(trees)):
        pending.append(("pass", k, (0, 0)))
        passed[k], given[k] = set(), 0
    finished = 0
    while finished < len(trees):
        ready = {}
        for e in pending:
            kind, k, o = e
            if kind == "pass":
                ready[e] = arrived[k, o] if o != (0, 0) else arrivals[k]
            elif kind == "sum":
                ready[e] = max([summed[k, c] for c in trees[k].children[o]], default=0.0)
            else:
                ready[e] = 0.0

        def rank(e):
            kind, k, o = e
            late = -trees[k].depth[o] if kind == "sum" else 0
            return ({"pass": 0, "sum": 0, "finish": 1}.get(kind, 2), urgency[k], late, str(o))

        able = [e for e in pending if ready[e] <= now + 1e-9]
        if able:
            e = min(able, key=rank)
        else:
            e = min(pending, key=lambda e: (ready[e], rank(e)))
        pending.remove(e)
        now = max(now, ready[e])
        steps.append(e)
        kind, k, o = e
        tree = trees[k]
        if kind == "pass":
            for c in tree.children[o]:
                arrived[k, c] = sent(o, c)
                pending.append(("pass", k, c))
            now += 0.03
            passed[k].add(o)
            while given[k] < len(tree.groups) and passed[k].issuperset(tree.groups[given[k]]):
                pending.append(("multiply", k, given[k]))
                given[k] += 1
        elif kind == "multiply":
            now += 0.15
            if given[k] == len(tree.groups) and not any(e[:2] == (kind, k) for e in pending):
                pending.append(("finish", k, 0))
        elif kind == "finish":
            now += 0.5
            pending += [("sum", k, c) for c in tree.order if not tree.children[c]]
        else:
            now += 0.05 if tree.children[o] else 0.02
            if o == (0, 0):
                finished += 1
            else:
                p = tree.parent[o]
                summed[k, o] = sent(o, p)
                if all((k, c) in summed for c in tree.children[p]):
                    pending.append(("sum", k, p))
    return steps


def layer_kernel(
    ns,
    nx,
    ny,
    *refs,
):
    sources, (out_ref, *scratch) = refs[:14], refs[14:]
    (
        residual_ref,
        value_ref,
        gate_ref,
        taps_ref,
        conv_bias_ref,
        ln_gain_ref,
        ln_bias_ref,
        out_weight,
        norm_gain_ref,
        ids_ref,
        route_weight_ref,
        expert_gate,
        expert_up,
        expert_down,
    ) = scratch[:14]
    (
        halo,
        gated,
        padded,
        stat,
        act,
        mixed,
        picks,
        places,
        route_cols,
        outgoing,
        xbuf,
        acc_gate,
        acc_up,
        acc_sq,
        partial,
        rs_in,
        rs_out,
        ret_out,
        ret_in,
        met,
        load_sem,
        halo_s,
        halo_r,
        stat_s,
        stat_r,
        act_s,
        act_r,
        z_s,
        z_r,
        ag_s,
        ag_r,
        rs_s,
        rs_r,
        rt_s,
        rt_r,
    ) = scratch[14:]
    ntp = nx * ny
    rows, width = residual_ref.shape
    total_width = ntp * width
    slots = places.shape[0]
    cap = slots // ns
    chunks = outgoing.shape[0]
    depth_rows = slots // chunks
    per_side = ns // (2 * chunks)
    taps = taps_ref.shape[0]
    reach = taps // 2
    edge = halo.shape[1]
    s = lax.axis_index("sp")
    t = lax.axis_index("tp")
    ty, tx = t // nx, lax.rem(t, nx)
    trees = [Tree(nx, ny, KINDS[k], k) for k in range(chunks)]
    offsets = sorted(trees[0].order, key=lambda o: (abs(signed(o[0], nx)) + abs(signed(o[1], ny)), o))
    number = {o: i for i, o in enumerate(offsets)}

    def tp_at(dx, dy):
        return lax.rem(ty + dy + 2 * ny, ny) * nx + lax.rem(tx + dx + 2 * nx, nx)

    def owner(o):
        return tp_at(-o[0], -o[1])

    def sp_at(d):
        return lax.rem(s + d + 2 * ns, ns)

    def distance(k, jj):
        return k * per_side + jj if jj < per_side else jj - (k + 2) * per_side

    def meet(r):
        if r > 0 and 2 ** (r - 1) < ns // 2:
            pl.semaphore_wait(met.at[r - 1], 2)
        if 2**r < ns // 2:
            for d in (2**r, -(2**r)):
                pl.semaphore_signal(
                    met.at[r], inc=1, device_id=(sp_at(d), t), device_id_type=MESH
                )

    def send(src, dst, send_sem, recv_sem, device):
        copy = pltpu.make_async_remote_copy(
            src_ref=src,
            dst_ref=dst,
            send_sem=send_sem,
            recv_sem=recv_sem,
            device_id=device,
            device_id_type=MESH,
        )
        copy.start()
        return copy

    with jax.named_scope("signal"):
        barrier = pltpu.get_barrier_semaphore()
        for i in range(1, ntp):
            pl.semaphore_signal(
                barrier, inc=1, device_id=(s, lax.rem(t + i, ntp)), device_id_type=MESH
            )
        for d in (1, -1):
            pl.semaphore_signal(barrier, inc=1, device_id=(sp_at(d), t), device_id_type=MESH)

        loads = {}
        for i in (1, 2, 9, 3, 4, 5, 6, 8, 10, 0, 7, 11, 12, 13):
            source = sources[i].at[0] if i >= 11 else sources[i]
            loads[i] = pltpu.make_async_copy(source, scratch[i], load_sem.at[i])
        for load in loads.values():
            load.start()

    with jax.named_scope("local"):
        loads[1].wait()
        loads[2].wait()
        gated_f = value_ref[...].astype(F32) * jax.nn.sigmoid(gate_ref[...].astype(F32))
        gated[...] = gated_f.astype(BF16)
        padded[edge : edge + rows, :] = gated[...].astype(F32)

        for i in (9, 3, 4, 5, 6, 8, 10, 0):
            loads[i].wait()
        expert_of = lax.broadcasted_iota(jnp.int32, (ns, rows), 0)
        chosen = [
            jnp.where(ids_ref[k : k + 1, :] == expert_of, 1.0, 0.0).astype(BF16)
            for k in range(TOPK)
        ]
        earlier = jnp.where(
            lax.broadcasted_iota(jnp.int32, (rows, rows), 0)
            < lax.broadcasted_iota(jnp.int32, (rows, rows), 1),
            1.0,
            0.0,
        ).astype(BF16)
        rank = jnp.dot(chosen[0] + chosen[1], earlier, preferred_element_type=F32).astype(BF16)
        slot = lax.broadcasted_iota(jnp.int32, (slots, ns), 0)
        in_chunk = (slot // cap) & (2 * per_side - 1)
        chunk_of = slot // depth_rows
        away = in_chunk + chunk_of * per_side
        away = jnp.where(in_chunk >= per_side, away - (2 * chunk_of + 2) * per_side, away)
        spread = jnp.where(
            lax.broadcasted_iota(jnp.int32, (slots, ns), 1) == ((s + away + 2 * ns) & (ns - 1)),
            1.0,
            0.0,
        ).astype(BF16)
        rank_at = jnp.dot(spread, rank, preferred_element_type=F32)
        slot_rank = (lax.broadcasted_iota(jnp.int32, (slots, rows), 0) & (cap - 1)).astype(F32)
        hit = rank_at == slot_rank
        both = jnp.zeros((slots, rows), F32)
        for k in range(TOPK):
            here = jnp.dot(spread, chosen[k], preferred_element_type=F32)
            here = jnp.where(hit, here, 0.0)
            picks[k] = here.T.astype(BF16)
            both = both + here
            route_cols[k] = jnp.broadcast_to(route_weight_ref[k : k + 1, :], (width, rows)).T
        places[...] = both.astype(BF16)

    with jax.named_scope("barrier"):
        pl.semaphore_wait(barrier, ntp - 1 + 2)
        meet(0)

    with jax.named_scope("halo"):
        to_right = send(
            gated.at[pl.ds(rows - edge, edge)], halo.at[0], halo_s.at[0], halo_r.at[0], (sp_at(1), t)
        )
        to_left = send(gated.at[pl.ds(0, edge)], halo.at[1], halo_s.at[1], halo_r.at[1], (sp_at(-1), t))
        pending = [to_right, to_left]
        meet(1)
        to_right.wait_recv()
        to_left.wait_recv()
        meet(2)
        padded[0:edge, :] = jnp.where(s > 0, halo[0].astype(F32), 0.0)
        padded[edge + rows : edge + rows + edge, :] = jnp.where(
            s < ns - 1, halo[1].astype(F32), 0.0
        )
    with jax.named_scope("conv"):
        tap_values = taps_ref[...].astype(F32)
        conv = jnp.zeros((rows, width), F32) + conv_bias_ref[...]
        for tap in range(taps):
            start = edge - reach + tap
            conv = conv + padded[start : start + rows, :] * tap_values[tap : tap + 1, :]
        conv_t = conv.T
        stat[t] = jnp.concatenate(
            [
                jnp.sum(conv_t, axis=0, keepdims=True),
                jnp.sum(conv_t * conv_t, axis=0, keepdims=True),
                1.0 / norm_gain_ref[...],
                ln_gain_ref[...],
                ln_bias_ref[...],
                jnp.zeros((3, width), F32),
            ],
            axis=0,
        )
        stat_copies = []
        for o in reversed(offsets[1:]):
            i = number[o]
            stat_copies.append(
                send(stat.at[t], stat.at[t], stat_s.at[i], stat_r.at[i], (s, tp_at(*o)))
            )
        own_mean = jnp.sum(conv, axis=1, keepdims=True) * (1.0 / width)
        act[0] = (conv - own_mean).astype(BF16)
        act_copies = {}
        for o in reversed(offsets[1:]):
            i = number[o]
            act_copies[o] = send(
                act.at[0], act.at[i], act_s.at[i], act_r.at[i], (s, tp_at(*o))
            )
    with jax.named_scope("stats"):
        meet(3)
        for copy in stat_copies:
            copy.wait_recv()
        pending += stat_copies + list(act_copies.values())
        totals = jnp.sum(stat[...], axis=0) * (1.0 / total_width)
        mean = totals[0:1, :]
        spread_inv = lax.rsqrt(totals[1:2, :] - mean * mean + 1e-05)
        lifts = [
            (stat[owner(o), 0:1, :] * (1.0 / width) - mean) * spread_inv for o in offsets
        ]
        lifts.append(spread_inv)
        lifts.append(jnp.zeros((rows - len(lifts), rows), F32))
        columns = jnp.concatenate(lifts, axis=0).T
        inv_col = columns[:, ntp : ntp + 1]
        total = residual_ref[...].astype(F32)
        loads[7].wait()
    with jax.named_scope("act_gather"):
        waiting = [(0, 0)] + list(reversed(offsets[1:]))
        half = len(waiting) // 2
        for group in (waiting[:half], waiting[half:]):
            blocks, tall = [], []
            for o in group:
                i = number[o]
                who = owner(o)
                if i:
                    act_copies[o].wait_recv()
                value = act[i].astype(F32) * inv_col + columns[:, i : i + 1]
                value = value * stat[who, 3:4, :] + stat[who, 4:5, :]
                blocks.append(jax.nn.silu(value).astype(BF16))
                tall.append(out_weight[pl.ds(pl.multiple_of(who * width, width), width), :])
            total = total + jnp.dot(
                jnp.concatenate(blocks, axis=1),
                jnp.concatenate(tall, axis=0),
                preferred_element_type=F32,
            )
    with jax.named_scope("project"):
        meet(4)
        mixed[...] = total
        scaled_rows = (total * norm_gain_ref[...]).astype(BF16)

    with jax.named_scope("dispatch"):
        dispatch = {}
        for k in SEND_ORDER:
            outgoing[k] = jnp.dot(
                places[k * depth_rows : (k + 1) * depth_rows, :],
                scaled_rows,
                preferred_element_type=F32,
            ).astype(BF16)
            for jj in range(2 * per_side):
                d = distance(k, jj)
                part = pl.ds(jj * cap, cap)
                if d == 0:
                    xbuf[k, 0, part, :] = outgoing[k, part, :]
                else:
                    dispatch[k, jj] = send(
                        outgoing.at[k, part],
                        xbuf.at[k, 0, part],
                        z_s.at[k, jj],
                        z_r.at[k, jj],
                        (sp_at(d), t),
                    )
        pending += list(dispatch.values())
        for i in (11, 12, 13):
            loads[i].wait()

    gathers, sums, returns = {}, {}, {}

    def pass_on(k, o):
        if o == (0, 0):
            for (kk, _), copy in dispatch.items():
                if kk == k:
                    copy.wait_recv()
        else:
            gathers[k, o].wait_recv()
        for c in trees[k].children[o]:
            gathers[k, c] = send(
                xbuf.at[k, number[o]],
                xbuf.at[k, number[c]],
                ag_s.at[k, number[c]],
                ag_r.at[k, number[c]],
                (s, tp_at(c[0] - o[0], c[1] - o[1])),
            )

    def multiply(k, index):
        group, first = trees[k].groups[index], index == 0
        blocks = [xbuf[k, number[o]] for o in group]
        owners = [owner(o) for o in group]
        wide = jnp.concatenate(blocks, axis=1)
        squares = None if first else acc_sq[k]
        for block, who in zip(blocks, owners):
            plain = block.astype(F32) * stat[who, 2:3, :]
            squares = plain * plain if squares is None else squares + plain * plain
        acc_sq[k] = squares
        for weight, acc in ((expert_gate, acc_gate), (expert_up, acc_up)):
            tall = jnp.concatenate(
                [weight[pl.ds(pl.multiple_of(who * width, width), width), :] for who in owners],
                axis=0,
            )
            product = jnp.dot(wide, tall, preferred_element_type=F32)
            acc[k] = product if first else acc[k] + product

    def finish_rows(k):
        square = jnp.sum(acc_sq[k], axis=1, keepdims=True) * (1.0 / total_width)
        scale = lax.rsqrt(square + 1e-06)
        hidden = (jax.nn.silu(acc_gate[k] * scale) * (acc_up[k] * scale)).astype(BF16)
        for i in range(ntp):
            partial[k, i] = jnp.dot(
                hidden, expert_down[:, i * width : (i + 1) * width], preferred_element_type=F32
            ).astype(BF16)

    def sum_up(k, o):
        who = owner(o)
        source = partial.at[k, who]
        if trees[k].children[o]:
            value = partial[k, who].astype(F32)
            for c in trees[k].children[o]:
                sums[k, c].wait_recv()
                value = value + rs_in[k, number[c]].astype(F32)
            if o == (0, 0):
                ret_out[k] = value.astype(BF16)
                return
            rs_out[k, number[o]] = value.astype(BF16)
            source = rs_out.at[k, number[o]]
        p = trees[k].parent[o]
        sums[k, o] = send(
            source,
            rs_in.at[k, number[o]],
            rs_s.at[k, number[o]],
            rs_r.at[k, number[o]],
            (s, tp_at(p[0] - o[0], p[1] - o[1])),
        )

    def give_back(k):
        for jj in range(2 * per_side):
            d = distance(k, jj)
            part = pl.ds(jj * cap, cap)
            if d == 0:
                ret_in[k, part, :] = ret_out[k, part, :]
            else:
                returns[k, jj] = send(
                    ret_out.at[k, part],
                    ret_in.at[k, part],
                    rt_s.at[k, jj],
                    rt_r.at[k, jj],
                    (sp_at(-d), t),
                )

    along = [5.6 * (2 * k + 1) / chunks**2 for k in range(chunks)]
    arrivals, clock = {}, 0.0
    for k in SEND_ORDER:
        clock += along[k]
        arrivals[k] = clock + 1.5 + 0.75 * (8 / chunks) * (k + 1)
    for kind, k, o in plan(trees, nx, ny, depth_rows, arrivals, URGENCY):
        with jax.named_scope(f"{kind}{k}{o}"):
            if kind == "pass":
                pass_on(k, o)
            elif kind == "multiply":
                multiply(k, o)
            elif kind == "finish":
                finish_rows(k)
            else:
                sum_up(k, o)
                if o == (0, 0):
                    give_back(k)
    with jax.named_scope("wait_back"):
        for copy in returns.values():
            copy.wait_recv()
    with jax.named_scope("result"):
        answer = jnp.concatenate([ret_in[k] for k in range(chunks)], axis=0)
        result = mixed[...]
        for k in range(TOPK):
            picked = jnp.dot(picks[k], answer, preferred_element_type=F32)
            result = result + picked * route_cols[k]
        out_ref[...] = result.astype(BF16)

    pending += list(gathers.values()) + list(sums.values()) + list(returns.values())
    for copy in pending:
        copy.wait_send()


def on_device(ns, nx, ny, *args):
    (
        residual,
        glu_value,
        glu_gate,
        conv_weight,
        conv_bias,
        ln_gain,
        ln_bias,
        out_weight,
        norm_gain,
        route_ids,
        route_weight,
        expert_gate,
        expert_up,
        expert_down,
    ) = args
    ntp = nx * ny
    rows, width = residual.shape
    hidden = expert_gate.shape[2]
    capacity = 2 * rows * TOPK // ns
    slots = ns * capacity
    k, rc = CHUNKS, slots // CHUNKS
    edge = 16
    row = lambda v: v.reshape(1, -1)
    vmem = pl.BlockSpec(memory_space=pltpu.VMEM)
    hbm = pl.BlockSpec(memory_space=pltpu.HBM)
    dma = pltpu.SemaphoreType.DMA
    operands = (
        residual,
        glu_value,
        glu_gate,
        conv_weight,
        row(conv_bias),
        row(ln_gain),
        row(ln_bias),
        out_weight,
        row(norm_gain),
        route_ids.T,
        route_weight.T,
        expert_gate,
        expert_up,
        expert_down,
    )
    return pl.pallas_call(
        functools.partial(layer_kernel, ns, nx, ny),
        out_shape=jax.ShapeDtypeStruct(residual.shape, BF16),
        in_specs=[hbm] * 14,
        out_specs=vmem,
        scratch_shapes=[
            *[pltpu.VMEM(a.shape[-2:], a.dtype) for a in operands],
            pltpu.VMEM((2, edge, width), BF16),
            pltpu.VMEM((rows, width), BF16),
            pltpu.VMEM((rows + 2 * edge, width), F32),
            pltpu.VMEM((ntp, 8, width), F32),
            pltpu.VMEM((ntp, rows, width), BF16),
            pltpu.VMEM((rows, width), F32),
            pltpu.VMEM((TOPK, rows, slots), BF16),
            pltpu.VMEM((slots, rows), BF16),
            pltpu.VMEM((TOPK, rows, width), F32),
            pltpu.VMEM((k, rc, width), BF16),
            pltpu.VMEM((k, ntp, rc, width), BF16),
            pltpu.VMEM((k, rc, hidden), F32),
            pltpu.VMEM((k, rc, hidden), F32),
            pltpu.VMEM((k, rc, width), F32),
            pltpu.VMEM((k, ntp, rc, width), BF16),
            pltpu.VMEM((k, ntp, rc, width), BF16),
            pltpu.VMEM((k, ntp, rc, width), BF16),
            pltpu.VMEM((k, rc, width), BF16),
            pltpu.VMEM((k, rc, width), BF16),
            pltpu.SemaphoreType.REGULAR((4,)),
            dma((14,)),
            dma((2,)),
            dma((2,)),
            dma((ntp,)),
            dma((ntp,)),
            dma((ntp,)),
            dma((ntp,)),
            dma((k, ns // k)),
            dma((k, ns // k)),
            dma((k, ntp)),
            dma((k, ntp)),
            dma((k, ntp)),
            dma((k, ntp)),
            dma((k, ns // k)),
            dma((k, ns // k)),
        ],
        compiler_params=pltpu.CompilerParams(
            collective_id=0, has_side_effects=True, vmem_limit_bytes=66 * 1000 * 1000
        ),
        name="layer",
    )(*operands)


IN_SPECS = (
    P("sp", "tp"),
    P("sp", "tp"),
    P("sp", "tp"),
    P(None, "tp"),
    P("tp"),
    P("tp"),
    P("tp"),
    P(None, "tp"),
    P("tp"),
    P("sp", None),
    P("sp", None),
    P("sp", None, "tp"),
    P("sp", None, "tp"),
    P("sp", "tp", None),
)


def solution(mesh, nx=NX):
    ns, ntp = mesh.shape["sp"], mesh.shape["tp"]
    return jax.shard_map(
        functools.partial(on_device, ns, nx, ntp // nx),
        mesh=mesh,
        in_specs=IN_SPECS,
        out_specs=P("sp", "tp"),
        check_vma=False,
    )
```

```python
import functools

import jax
import jax.numpy as jnp
from jax import lax
from jax.experimental import pallas as pl
from jax.experimental.pallas import tpu as pltpu
from jax.sharding import PartitionSpec as P

MESH = pl.DeviceIdType.MESH
TOPK = 2
F32 = jnp.float32
BF16 = jnp.bfloat16
NX = 4
CHUNKS = 8
SEND_ORDER = (4, 5, 6, 3, 0, 7, 2, 1)
URGENCY = (7, 3, 5, 2, 4, 0, 6, 1)
KINDS = (0, 0, 0, 0, 1, 0, 1, 1)

TREE_4X4 = {
    (1, 0): (0, 0),
    (3, 0): (0, 0),
    (0, 1): (0, 0),
    (0, 3): (0, 0),
    (1, 1): (1, 0),
    (3, 1): (0, 1),
    (3, 3): (3, 0),
    (1, 3): (0, 3),
    (2, 0): (1, 0),
    (0, 2): (0, 3),
    (2, 1): (3, 1),
    (2, 3): (1, 3),
    (1, 2): (1, 1),
    (3, 2): (3, 3),
    (2, 2): (2, 1),
}
SHALLOW_4X4 = {
    **{o: (0, 0) for o in TREE_4X4},
    (2, 0): (1, 0),
    (0, 2): (0, 3),
    (2, 1): (1, 1),
    (2, 3): (3, 3),
    (1, 2): (1, 3),
    (3, 2): (3, 1),
    (2, 2): (1, 1),
}


def turned(tree, quarters):
    def turn(o):
        for _ in range(quarters):
            o = (-o[1] % 4, o[0])
        return o

    return {turn(c): turn(p) for c, p in tree.items()}


class Tree:
    def __init__(self, nx, ny, kind, quarters):
        if (nx, ny) == (4, 4):
            parent = turned(SHALLOW_4X4 if kind else TREE_4X4, quarters)
        else:
            parent, frontier = {}, [(0, 0)]
            while frontier:
                grown = []
                for px, py in frontier:
                    for dx, dy in ((1, 0), (nx - 1, 0), (0, 1), (0, ny - 1)):
                        o = ((px + dx) % nx, (py + dy) % ny)
                        if o != (0, 0) and o not in parent:
                            parent[o] = (px, py)
                            grown.append(o)
                frontier = grown
        self.parent = parent
        self.depth = {(0, 0): 0}
        self.order = [(0, 0)]
        for o in self.order:
            for c in sorted(parent):
                if parent[c] == o:
                    self.depth[c] = self.depth[o] + 1
                    self.order.append(c)
        self.children = {o: [c for c in self.order if parent.get(c) == o] for o in self.order}
        self.groups = [
            [o for o in self.order if low <= self.depth[o] <= high]
            for low, high in ((0, 1), (2, 2), (3, 9))
        ]
        self.groups = [g for g in self.groups if g]
        self.relays = [o for o in self.order if self.children[o]]
        self.lane = {o: i for i, o in enumerate(self.relays)}
        self.group_of = {o: i for i, g in enumerate(self.groups) for o in g}


def signed(v, n):
    return (v + n // 2 - 1) % n - (n // 2 - 1)


def plan(trees, nx, ny, rows, arrivals, urgency):
    wire, latency, hop = rows * 256 / 46.65e3, 2.2, 0.75
    link, now, steps, pending = {}, 0.0, [], []
    arrived, summed, passed, given = {}, {}, {}, {}

    def sent(p, o):
        dx, dy = signed(o[0] - p[0], nx), signed(o[1] - p[1], ny)
        end = now
        for axis, v, n in ((0, dx, nx), (1, dy, ny)):
            if v:
                for way in (1, -1) if 2 * v == n else (1 if v > 0 else -1,):
                    link[axis, way] = max(link.get((axis, way), 0.0), now) + wire
                    end = max(end, link[axis, way])
        return end + latency + hop * (abs(dx) + abs(dy) - 1)

    for k in range(len(trees)):
        pending.append(("pass", k, (0, 0)))
        passed[k], given[k] = set(), 0
    finished = 0
    while finished < len(trees):
        ready = {}
        for e in pending:
            kind, k, o = e
            if kind == "pass":
                ready[e] = arrived[k, o] if o != (0, 0) else arrivals[k]
            elif kind == "sum":
                ready[e] = max([summed[k, c] for c in trees[k].children[o]], default=0.0)
            else:
                ready[e] = 0.0

        def rank(e):
            kind, k, o = e
            late = -trees[k].depth[o] if kind == "sum" else 0
            return ({"pass": 0, "sum": 0, "finish": 1}.get(kind, 2), urgency[k], late, str(o))

        able = [e for e in pending if ready[e] <= now + 1e-9]
        if able:
            e = min(able, key=rank)
        else:
            e = min(pending, key=lambda e: (ready[e], rank(e)))
        pending.remove(e)
        now = max(now, ready[e])
        steps.append(e)
        kind, k, o = e
        tree = trees[k]
        if kind == "pass":
            for c in tree.children[o]:
                arrived[k, c] = sent(o, c)
                pending.append(("pass", k, c))
            now += 0.03
            passed[k].add(o)
            while given[k] < len(tree.groups) and passed[k].issuperset(tree.groups[given[k]]):
                pending.append(("multiply", k, given[k]))
                given[k] += 1
        elif kind == "multiply":
            now += 0.02 + 0.001 * rows
            if given[k] == len(tree.groups) and not any(e[:2] == (kind, k) for e in pending):
                pending.append(("finish", k, 0))
        elif kind == "finish":
            now += 0.1 + 0.003 * rows
            pending += [("sum", k, c) for c in tree.order if not tree.children[c]]
        else:
            now += 0.05 if tree.children[o] else 0.02
            if o == (0, 0):
                finished += 1
            else:
                p = tree.parent[o]
                summed[k, o] = sent(o, p)
                if all((k, c) in summed for c in tree.children[p]):
                    pending.append(("sum", k, p))
    return steps


def layer_kernel(
    ns,
    nx,
    ny,
    *refs,
):
    sources, (out_ref, *scratch) = refs[:14], refs[14:]
    (
        residual_ref,
        value_ref,
        gate_ref,
        taps_ref,
        conv_bias_ref,
        ln_gain_ref,
        ln_bias_ref,
        out_weight,
        norm_gain_ref,
        ids_ref,
        route_weight_ref,
        expert_gate,
        expert_up,
        expert_down,
    ) = scratch[:14]
    (
        halo,
        gated,
        padded,
        stat,
        act,
        mixed,
        picks,
        places,
        route_cols,
        outgoing,
        xbuf,
        acc_gate,
        acc_up,
        acc_sq,
        partial,
        rs_in,
        rs_out,
        ret_out,
        ret_in,
        met,
        load_sem,
        halo_s,
        halo_r,
        stat_s,
        stat_r,
        act_s,
        act_r,
        z_s,
        z_r,
        ag_s,
        ag_r,
        leaf_r,
        rs_s,
        rs_r,
        rt_s,
        rt_r,
    ) = scratch[14:]
    ntp = nx * ny
    rows, width = residual_ref.shape
    total_width = ntp * width
    slots = places.shape[0]
    cap = slots // ns
    chunks = xbuf.shape[0]
    depth_rows = slots // chunks
    per_side = ns // (2 * chunks)
    taps = taps_ref.shape[0]
    reach = taps // 2
    edge = halo.shape[1]
    s = lax.axis_index("sp")
    t = lax.axis_index("tp")
    ty, tx = t // nx, lax.rem(t, nx)
    trees = [Tree(nx, ny, KINDS[k], k) for k in range(chunks)]
    offsets = sorted(trees[0].order, key=lambda o: (abs(signed(o[0], nx)) + abs(signed(o[1], ny)), o))
    number = {o: i for i, o in enumerate(offsets)}

    def tp_at(dx, dy):
        return lax.rem(ty + dy + 2 * ny, ny) * nx + lax.rem(tx + dx + 2 * nx, nx)

    def owner(o):
        return tp_at(-o[0], -o[1])

    def sp_at(d):
        return lax.rem(s + d + 2 * ns, ns)

    def distance(k, jj):
        return k * per_side + jj if jj < per_side else jj - (k + 2) * per_side

    def meet(r):
        if r > 0 and 2 ** (r - 1) < ns // 2:
            pl.semaphore_wait(met.at[r - 1], 2)
        if 2**r < ns // 2:
            for d in (2**r, -(2**r)):
                pl.semaphore_signal(
                    met.at[r], inc=1, device_id=(sp_at(d), t), device_id_type=MESH
                )

    def all_of(ref, sem):
        return pltpu.make_async_copy(ref, ref, sem)

    def send(src, dst, send_sem, recv_sem, device):
        copy = pltpu.make_async_remote_copy(
            src_ref=src,
            dst_ref=dst,
            send_sem=send_sem,
            recv_sem=recv_sem,
            device_id=device,
            device_id_type=MESH,
        )
        copy.start()
        return copy

    with jax.named_scope("signal"):
        barrier = pltpu.get_barrier_semaphore()
        for i in range(1, ntp):
            pl.semaphore_signal(
                barrier, inc=1, device_id=(s, lax.rem(t + i, ntp)), device_id_type=MESH
            )
        for d in (1, -1):
            pl.semaphore_signal(barrier, inc=1, device_id=(sp_at(d), t), device_id_type=MESH)

        loads = {}
        for i in (1, 2, 9, 3, 4, 5, 6, 8, 10, 0, 7, 11, 12, 13):
            source = sources[i].at[0] if i >= 11 else sources[i]
            loads[i] = pltpu.make_async_copy(source, scratch[i], load_sem.at[i])
        for load in loads.values():
            load.start()

    with jax.named_scope("local"):
        loads[1].wait()
        loads[2].wait()
        gated_f = value_ref[...].astype(F32) * jax.nn.sigmoid(gate_ref[...].astype(F32))
        gated[...] = gated_f.astype(BF16)
        padded[edge : edge + rows, :] = gated[...].astype(F32)

    with jax.named_scope("barrier"):
        pl.semaphore_wait(barrier, ntp - 1 + 2)
        meet(0)

    with jax.named_scope("halo"):
        for side, start, d in ((0, rows - edge, 1), (1, 0, -1)):
            send(
                gated.at[pl.ds(start, edge)],
                halo.at[side],
                halo_s.at[0],
                halo_r.at[0],
                (sp_at(d), t),
            )
        meet(1)
        all_of(halo, halo_r.at[0]).wait()
        meet(2)
        padded[0:edge, :] = jnp.where(s > 0, halo[0].astype(F32), 0.0)
        padded[edge + rows : edge + rows + edge, :] = jnp.where(
            s < ns - 1, halo[1].astype(F32), 0.0
        )
    with jax.named_scope("conv"):
        for i in (3, 4, 5, 6, 8):
            loads[i].wait()
        tap_values = taps_ref[...].astype(F32)
        conv = jnp.zeros((rows, width), F32) + conv_bias_ref[...]
        for tap in range(taps):
            start = edge - reach + tap
            conv = conv + padded[start : start + rows, :] * tap_values[tap : tap + 1, :]
        conv_t = conv.T
        stat[t] = jnp.concatenate(
            [
                jnp.sum(conv_t, axis=0, keepdims=True),
                jnp.sum(conv_t * conv_t, axis=0, keepdims=True),
                1.0 / norm_gain_ref[...],
                ln_gain_ref[...],
                ln_bias_ref[...],
                jnp.zeros((3, width), F32),
            ],
            axis=0,
        )
        far_first = list(reversed(offsets[1:]))
        for o in far_first:
            send(stat.at[t], stat.at[t], stat_s.at[0], stat_r.at[0], (s, tp_at(*o)))
        own_mean = jnp.sum(conv, axis=1, keepdims=True) * (1.0 / width)
        act[0] = (conv - own_mean).astype(BF16)
        half = ntp // 2
        for n, o in enumerate(far_first):
            sem = act_r.at[0 if n + 1 < half else 1]
            send(act.at[0], act.at[number[o]], act_s.at[0], sem, (s, tp_at(*o)))
    with jax.named_scope("route"):
        meet(3)
        for i in (9, 10, 0):
            loads[i].wait()
        expert_of = lax.broadcasted_iota(jnp.int32, (ns, rows), 0)
        chosen = [
            jnp.where(ids_ref[k : k + 1, :] == expert_of, 1.0, 0.0).astype(BF16)
            for k in range(TOPK)
        ]
        earlier = jnp.where(
            lax.broadcasted_iota(jnp.int32, (rows, rows), 0)
            < lax.broadcasted_iota(jnp.int32, (rows, rows), 1),
            1.0,
            0.0,
        ).astype(BF16)
        rank = jnp.dot(chosen[0] + chosen[1], earlier, preferred_element_type=F32).astype(BF16)
        slot = lax.broadcasted_iota(jnp.int32, (slots, ns), 0)
        in_chunk = (slot // cap) & (2 * per_side - 1)
        chunk_of = slot // depth_rows
        away = in_chunk + chunk_of * per_side
        away = jnp.where(in_chunk >= per_side, away - (2 * chunk_of + 2) * per_side, away)
        spread = jnp.where(
            lax.broadcasted_iota(jnp.int32, (slots, ns), 1) == ((s + away + 2 * ns) & (ns - 1)),
            1.0,
            0.0,
        ).astype(BF16)
        rank_at = jnp.dot(spread, rank, preferred_element_type=F32)
        slot_rank = (lax.broadcasted_iota(jnp.int32, (slots, rows), 0) & (cap - 1)).astype(F32)
        hit = rank_at == slot_rank
        both = jnp.zeros((slots, rows), F32)
        for k in range(TOPK):
            here = jnp.dot(spread, chosen[k], preferred_element_type=F32)
            here = jnp.where(hit, here, 0.0)
            picks[k] = here.T.astype(BF16)
            both = both + here
            route_cols[k] = jnp.broadcast_to(route_weight_ref[k : k + 1, :], (width, rows)).T
        places[...] = both.astype(BF16)
    with jax.named_scope("stats"):
        all_of(stat.at[pl.ds(0, ntp - 1)], stat_r.at[0]).wait()
        totals = jnp.sum(stat[...], axis=0) * (1.0 / total_width)
        mean = totals[0:1, :]
        spread_inv = lax.rsqrt(totals[1:2, :] - mean * mean + 1e-05)
        lifts = [
            (stat[owner(o), 0:1, :] * (1.0 / width) - mean) * spread_inv for o in offsets
        ]
        lifts.append(spread_inv)
        lifts.append(jnp.zeros((rows - len(lifts), rows), F32))
        columns = jnp.concatenate(lifts, axis=0).T
        inv_col = columns[:, ntp : ntp + 1]
        total = residual_ref[...].astype(F32)
        loads[7].wait()
    with jax.named_scope("act_gather"):
        waiting = [(0, 0)] + far_first
        for n, group in enumerate((waiting[:half], waiting[half:])):
            blocks, tall = [], []
            if n == 1 or half > 1:
                all_of(act.at[pl.ds(0, half - 1 + n)], act_r.at[n]).wait()
            for o in group:
                i = number[o]
                who = owner(o)
                value = act[i].astype(F32) * inv_col + columns[:, i : i + 1]
                value = value * stat[who, 3:4, :] + stat[who, 4:5, :]
                blocks.append(jax.nn.silu(value).astype(BF16))
                tall.append(out_weight[pl.ds(pl.multiple_of(who * width, width), width), :])
            total = total + jnp.dot(
                jnp.concatenate(blocks, axis=1),
                jnp.concatenate(tall, axis=0),
                preferred_element_type=F32,
            )
    with jax.named_scope("project"):
        meet(4)
        mixed[...] = total
        scaled_rows = (total * norm_gain_ref[...]).astype(BF16)

    with jax.named_scope("dispatch"):
        for k in SEND_ORDER:
            chunk = pl.ds(k * depth_rows, depth_rows)
            outgoing[chunk, :] = jnp.dot(
                places[chunk, :], scaled_rows, preferred_element_type=F32
            ).astype(BF16)
            for jj in range(2 * per_side):
                d = distance(k, jj)
                part, flat = pl.ds(jj * cap, cap), pl.ds(k * depth_rows + jj * cap, cap)
                if d == 0:
                    xbuf[k, 0, part, :] = outgoing[flat, :]
                else:
                    send(
                        outgoing.at[flat], xbuf.at[k, 0, part], z_s.at[0], z_r.at[k], (sp_at(d), t)
                    )
        for i in (11, 12, 13):
            loads[i].wait()

    def blocks_of(buffer, k, count):
        return buffer.at[k, pl.ds(0, count)]

    def arriving_leaves(k, index):
        tree = trees[k]
        return [o for o in tree.groups[index] if o != (0, 0) and not tree.children[o]]

    def pass_on(k, o):
        tree = trees[k]
        if o == (0, 0):
            here = cap if distance(k, 0) == 0 else 0
            all_of(xbuf.at[k, 0, pl.ds(0, depth_rows - here)], z_r.at[k]).wait()
        elif tree.children[o]:
            all_of(xbuf.at[k, number[o]], ag_r.at[k, tree.lane[o] - 1]).wait()
        for c in tree.children[o]:
            if tree.children[c]:
                sem = ag_r.at[k, tree.lane[c] - 1]
            else:
                sem = leaf_r.at[k, tree.group_of[c]]
            send(
                xbuf.at[k, number[o]],
                xbuf.at[k, number[c]],
                ag_s.at[0],
                sem,
                (s, tp_at(c[0] - o[0], c[1] - o[1])),
            )

    def multiply(k, index):
        group, first = trees[k].groups[index], index == 0
        leaves = arriving_leaves(k, index)
        if leaves:
            all_of(blocks_of(xbuf, k, len(leaves)), leaf_r.at[k, index]).wait()
        blocks = [xbuf[k, number[o]] for o in group]
        owners = [owner(o) for o in group]
        wide = jnp.concatenate(blocks, axis=1)
        squares = None if first else acc_sq[k]
        for block, who in zip(blocks, owners):
            plain = block.astype(F32) * stat[who, 2:3, :]
            squares = plain * plain if squares is None else squares + plain * plain
        acc_sq[k] = squares
        for weight, acc in ((expert_gate, acc_gate), (expert_up, acc_up)):
            tall = jnp.concatenate(
                [weight[pl.ds(pl.multiple_of(who * width, width), width), :] for who in owners],
                axis=0,
            )
            product = jnp.dot(wide, tall, preferred_element_type=F32)
            acc[k] = product if first else acc[k] + product

    def finish_rows(k):
        square = jnp.sum(acc_sq[k], axis=1, keepdims=True) * (1.0 / total_width)
        scale = lax.rsqrt(square + 1e-06)
        hidden = (jax.nn.silu(acc_gate[k] * scale) * (acc_up[k] * scale)).astype(BF16)
        for i in range(ntp):
            partial[k, i] = jnp.dot(
                hidden, expert_down[:, i * width : (i + 1) * width], preferred_element_type=F32
            ).astype(BF16)

    def sum_up(k, o):
        who = owner(o)
        tree = trees[k]
        source = partial.at[k, who]
        if tree.children[o]:
            count = len(tree.children[o])
            all_of(blocks_of(rs_in, k, count), rs_r.at[k, tree.lane[o]]).wait()
            value = partial[k, who].astype(F32)
            for c in tree.children[o]:
                value = value + rs_in[k, number[c]].astype(F32)
            if o == (0, 0):
                ret_out[pl.ds(k * depth_rows, depth_rows), :] = value.astype(BF16)
                return
            rs_out[k, number[o]] = value.astype(BF16)
            source = rs_out.at[k, number[o]]
        p = tree.parent[o]
        send(
            source,
            rs_in.at[k, number[o]],
            rs_s.at[0],
            rs_r.at[k, tree.lane[p]],
            (s, tp_at(p[0] - o[0], p[1] - o[1])),
        )

    def give_back(k):
        for jj in range(2 * per_side):
            d = distance(k, jj)
            part = pl.ds(k * depth_rows + jj * cap, cap)
            if d == 0:
                ret_in[part, :] = ret_out[part, :]
            else:
                send(ret_out.at[part], ret_in.at[part], rt_s.at[0], rt_r.at[0], (sp_at(-d), t))

    along = [5.6 * (2 * k + 1) / chunks**2 for k in range(chunks)]
    arrivals, clock = {}, 0.0
    for k in SEND_ORDER:
        clock += along[k]
        arrivals[k] = clock + 1.5 + 0.75 * (8 / chunks) * (k + 1)
    for kind, k, o in plan(trees, nx, ny, depth_rows, arrivals, URGENCY):
        with jax.named_scope(f"{kind}{k}{o}"):
            if kind == "pass":
                pass_on(k, o)
            elif kind == "multiply":
                multiply(k, o)
            elif kind == "finish":
                finish_rows(k)
            else:
                sum_up(k, o)
                if o == (0, 0):
                    give_back(k)
    away_rows = pl.ds(0, slots - cap)
    with jax.named_scope("wait_sends"):
        all_of(halo, halo_s.at[0]).wait()
        all_of(stat.at[pl.ds(0, ntp - 1)], stat_s.at[0]).wait()
        all_of(act.at[pl.ds(0, ntp - 1)], act_s.at[0]).wait()
        all_of(outgoing.at[away_rows], z_s.at[0]).wait()
        all_of(xbuf.at[:, pl.ds(0, ntp - 1)], ag_s.at[0]).wait()
        all_of(rs_in.at[:, pl.ds(0, ntp - 1)], rs_s.at[0]).wait()
    with jax.named_scope("wait_back"):
        all_of(ret_in.at[away_rows], rt_r.at[0]).wait()
    with jax.named_scope("result"):
        answer = ret_in[...]
        result = mixed[...]
        for k in range(TOPK):
            picked = jnp.dot(picks[k], answer, preferred_element_type=F32)
            result = result + picked * route_cols[k]
        out_ref[...] = result.astype(BF16)

    with jax.named_scope("end"):
        all_of(ret_out.at[away_rows], rt_s.at[0]).wait()


def on_device(ns, nx, ny, *args):
    (
        residual,
        glu_value,
        glu_gate,
        conv_weight,
        conv_bias,
        ln_gain,
        ln_bias,
        out_weight,
        norm_gain,
        route_ids,
        route_weight,
        expert_gate,
        expert_up,
        expert_down,
    ) = args
    ntp = nx * ny
    rows, width = residual.shape
    hidden = expert_gate.shape[2]
    capacity = 2 * rows * TOPK // ns
    slots = ns * capacity
    k, rc = CHUNKS, slots // CHUNKS
    edge = 16
    row = lambda v: v.reshape(1, -1)
    vmem = pl.BlockSpec(memory_space=pltpu.VMEM)
    hbm = pl.BlockSpec(memory_space=pltpu.HBM)
    dma = pltpu.SemaphoreType.DMA
    operands = (
        residual,
        glu_value,
        glu_gate,
        conv_weight,
        row(conv_bias),
        row(ln_gain),
        row(ln_bias),
        out_weight,
        row(norm_gain),
        route_ids.T,
        route_weight.T,
        expert_gate,
        expert_up,
        expert_down,
    )
    return pl.pallas_call(
        functools.partial(layer_kernel, ns, nx, ny),
        out_shape=jax.ShapeDtypeStruct(residual.shape, BF16),
        in_specs=[hbm] * 14,
        out_specs=vmem,
        scratch_shapes=[
            *[pltpu.VMEM(a.shape[-2:], a.dtype) for a in operands],
            pltpu.VMEM((2, edge, width), BF16),
            pltpu.VMEM((rows, width), BF16),
            pltpu.VMEM((rows + 2 * edge, width), F32),
            pltpu.VMEM((ntp, 8, width), F32),
            pltpu.VMEM((ntp, rows, width), BF16),
            pltpu.VMEM((rows, width), F32),
            pltpu.VMEM((TOPK, rows, slots), BF16),
            pltpu.VMEM((slots, rows), BF16),
            pltpu.VMEM((TOPK, rows, width), F32),
            pltpu.VMEM((slots, width), BF16),
            pltpu.VMEM((k, ntp, rc, width), BF16),
            pltpu.VMEM((k, rc, hidden), F32),
            pltpu.VMEM((k, rc, hidden), F32),
            pltpu.VMEM((k, rc, width), F32),
            pltpu.VMEM((k, ntp, rc, width), BF16),
            pltpu.VMEM((k, ntp, rc, width), BF16),
            pltpu.VMEM((k, ntp, rc, width), BF16),
            pltpu.VMEM((slots, width), BF16),
            pltpu.VMEM((slots, width), BF16),
            pltpu.SemaphoreType.REGULAR((4,)),
            dma((14,)),
            dma((1,)),
            dma((1,)),
            dma((1,)),
            dma((1,)),
            dma((1,)),
            dma((2,)),
            dma((1,)),
            dma((k,)),
            dma((1,)),
            dma((k, 9)),
            dma((k, 3)),
            dma((1,)),
            dma((k, 10)),
            dma((1,)),
            dma((1,)),
        ],
        compiler_params=pltpu.CompilerParams(
            collective_id=0, has_side_effects=True, vmem_limit_bytes=66 * 1000 * 1000
        ),
        name="layer",
    )(*operands)


IN_SPECS = (
    P("sp", "tp"),
    P("sp", "tp"),
    P("sp", "tp"),
    P(None, "tp"),
    P("tp"),
    P("tp"),
    P("tp"),
    P(None, "tp"),
    P("tp"),
    P("sp", None),
    P("sp", None),
    P("sp", None, "tp"),
    P("sp", None, "tp"),
    P("sp", "tp", None),
)


def solution(mesh, nx=NX):
    ns, ntp = mesh.shape["sp"], mesh.shape["tp"]
    return jax.shard_map(
        functools.partial(on_device, ns, nx, ntp // nx),
        mesh=mesh,
        in_specs=IN_SPECS,
        out_specs=P("sp", "tp"),
        check_vma=False,
    )
```

```python
import functools

import jax
import jax.numpy as jnp
from jax import lax
from jax.experimental import pallas as pl
from jax.experimental.pallas import tpu as pltpu
from jax.sharding import PartitionSpec as P

MESH = pl.DeviceIdType.MESH
TOPK = 2
F32 = jnp.float32
BF16 = jnp.bfloat16
NX = 4
CHUNKS = 8
SEND_ORDER = (1, 2, 3, 4, 0, 7, 6, 5)
URGENCY = (6, 2, 7, 5, 0, 4, 1, 3)
SUM_URGENCY = (6, 5, 7, 1, 3, 4, 2, 0)
KINDS = (0, 0, 1, 1, 0, 1, 1, 1)
LEAD = 0.3

TREE_4X4 = {
    (1, 0): (0, 0),
    (3, 0): (0, 0),
    (0, 1): (0, 0),
    (0, 3): (0, 0),
    (1, 1): (1, 0),
    (3, 1): (0, 1),
    (3, 3): (3, 0),
    (1, 3): (0, 3),
    (2, 0): (1, 0),
    (0, 2): (0, 3),
    (2, 1): (3, 1),
    (2, 3): (1, 3),
    (1, 2): (1, 1),
    (3, 2): (3, 3),
    (2, 2): (2, 1),
}
SHALLOW_4X4 = {
    **{o: (0, 0) for o in TREE_4X4},
    (2, 0): (1, 0),
    (0, 2): (0, 3),
    (2, 1): (1, 1),
    (2, 3): (3, 3),
    (1, 2): (1, 3),
    (3, 2): (3, 1),
    (2, 2): (1, 1),
}
DIRECT_4X4 = {o: (0, 0) for o in TREE_4X4}


def turned(tree, quarters):
    def turn(o):
        for _ in range(quarters):
            o = (-o[1] % 4, o[0])
        return o

    return {turn(c): turn(p) for c, p in tree.items()}


class Tree:
    def __init__(self, nx, ny, kind, quarters):
        if (nx, ny) == (4, 4):
            parent = turned((TREE_4X4, SHALLOW_4X4, DIRECT_4X4)[kind], quarters)
        else:
            parent, frontier = {}, [(0, 0)]
            while frontier:
                grown = []
                for px, py in frontier:
                    for dx, dy in ((1, 0), (nx - 1, 0), (0, 1), (0, ny - 1)):
                        o = ((px + dx) % nx, (py + dy) % ny)
                        if o != (0, 0) and o not in parent:
                            parent[o] = (px, py)
                            grown.append(o)
                frontier = grown
        self.parent = parent
        self.depth = {(0, 0): 0}
        self.order = [(0, 0)]
        for o in self.order:
            for c in sorted(parent):
                if parent[c] == o:
                    self.depth[c] = self.depth[o] + 1
                    self.order.append(c)
        self.children = {o: [c for c in self.order if parent.get(c) == o] for o in self.order}
        self.groups = [
            [o for o in self.order if low <= self.depth[o] <= high]
            for low, high in ((0, 1), (2, 2), (3, 9))
        ]
        self.groups = [g for g in self.groups if g]
        self.relays = [o for o in self.order if self.children[o]]
        self.lane = {o: i for i, o in enumerate(self.relays)}
        self.group_of = {o: i for i, g in enumerate(self.groups) for o in g}


def signed(v, n):
    return (v + n // 2 - 1) % n - (n // 2 - 1)


def plan(trees, nx, ny, rows, arrivals, urgency, sum_urgency, lead):
    wire, latency, hop = rows * 256 / 46.65e3, 2.2, 0.75
    link, now, steps, pending = {}, 0.0, [], []
    arrived, summed, passed, given = {}, {}, {}, {}

    def sent(p, o):
        dx, dy = signed(o[0] - p[0], nx), signed(o[1] - p[1], ny)
        end = now
        for axis, v, n in ((0, dx, nx), (1, dy, ny)):
            if v:
                for way in (1, -1) if 2 * v == n else (1 if v > 0 else -1,):
                    link[axis, way] = max(link.get((axis, way), 0.0), now) + wire
                    end = max(end, link[axis, way])
        return end + latency + hop * (abs(dx) + abs(dy) - 1)

    def way(p, o):
        dx, dy = signed(o[0] - p[0], nx), signed(o[1] - p[1], ny)
        return (0, 1 if dx > 0 else -1) if dx else (1, 1 if dy > 0 else -1)

    for k in range(len(trees)):
        pending.append(("pass", k, (0, 0)))
        passed[k], given[k] = set(), 0
    finished = 0
    while finished < len(trees):
        ready = {}
        for e in pending:
            kind, k, o = e
            if kind == "pass":
                ready[e] = arrived[k, o] if o != (0, 0) else arrivals[k]
                ways = [way(o, c) for c in trees[k].children[o]]
            elif kind == "sum":
                ready[e] = max([summed[k, c] for c in trees[k].children[o]], default=0.0)
                ways = [way(o, trees[k].parent[o])] if o != (0, 0) else []
            else:
                ready[e] = 0.0
                ways = []
            if ways:
                ready[e] = max(ready[e], min(link.get(w, 0.0) for w in ways) - lead)

        def rank(e):
            kind, k, o = e
            late = -trees[k].depth[o] if kind == "sum" else 0
            first = (sum_urgency if kind == "sum" else urgency)[k]
            return ({"pass": 0, "sum": 0, "finish": 1}.get(kind, 2), first, late, str(o))

        able = [e for e in pending if ready[e] <= now + 1e-9]
        if able:
            e = min(able, key=rank)
        else:
            e = min(pending, key=lambda e: (ready[e], rank(e)))
        pending.remove(e)
        now = max(now, ready[e])
        steps.append(e)
        kind, k, o = e
        tree = trees[k]
        if kind == "pass":
            for c in tree.children[o]:
                arrived[k, c] = sent(o, c)
                pending.append(("pass", k, c))
            now += 0.03
            passed[k].add(o)
            while given[k] < len(tree.groups) and passed[k].issuperset(tree.groups[given[k]]):
                pending.append(("multiply", k, given[k]))
                given[k] += 1
        elif kind == "multiply":
            now += 0.02 + 0.001 * rows
            if given[k] == len(tree.groups) and not any(e[:2] == (kind, k) for e in pending):
                pending.append(("finish", k, 0))
        elif kind == "finish":
            now += 0.1 + 0.003 * rows
            pending += [("sum", k, c) for c in tree.order if not tree.children[c]]
        else:
            now += 0.05 if tree.children[o] else 0.02
            if o == (0, 0):
                finished += 1
            else:
                p = tree.parent[o]
                summed[k, o] = sent(o, p)
                if all((k, c) in summed for c in tree.children[p]):
                    pending.append(("sum", k, p))
    return steps


def layer_kernel(
    ns,
    nx,
    ny,
    *refs,
):
    sources, (out_ref, *scratch) = refs[:14], refs[14:]
    (
        residual_ref,
        value_ref,
        gate_ref,
        taps_ref,
        conv_bias_ref,
        ln_gain_ref,
        ln_bias_ref,
        out_weight,
        norm_gain_ref,
        ids_ref,
        route_weight_ref,
        expert_gate,
        expert_up,
        expert_down,
    ) = scratch[:14]
    (
        halo,
        gated,
        padded,
        stat,
        gains,
        act,
        mixed,
        picks,
        places,
        route_cols,
        outgoing,
        xbuf,
        acc_gate,
        acc_up,
        acc_sq,
        partial,
        rs_in,
        rs_out,
        ret_out,
        ret_in,
        met,
        load_sem,
        halo_s,
        halo_r,
        stat_s,
        stat_r,
        act_s,
        act_r,
        z_s,
        z_r,
        ag_s,
        ag_r,
        leaf_r,
        rs_s,
        rs_r,
        rt_s,
        rt_r,
    ) = scratch[14:]
    ntp = nx * ny
    rows, width = residual_ref.shape
    total_width = ntp * width
    slots = places.shape[0]
    cap = slots // ns
    chunks = xbuf.shape[0]
    depth_rows = slots // chunks
    per_side = ns // (2 * chunks)
    taps = taps_ref.shape[0]
    reach = taps // 2
    edge = halo.shape[1]
    s = lax.axis_index("sp")
    t = lax.axis_index("tp")
    ty, tx = t // nx, lax.rem(t, nx)
    trees = [Tree(nx, ny, KINDS[k], k) for k in range(chunks)]
    offsets = sorted(trees[0].order, key=lambda o: (abs(signed(o[0], nx)) + abs(signed(o[1], ny)), o))
    number = {o: i for i, o in enumerate(offsets)}

    def tp_at(dx, dy):
        return lax.rem(ty + dy + 2 * ny, ny) * nx + lax.rem(tx + dx + 2 * nx, nx)

    def owner(o):
        return tp_at(-o[0], -o[1])

    def sp_at(d):
        return lax.rem(s + d + 2 * ns, ns)

    def distance(k, jj):
        return k * per_side + jj if jj < per_side else jj - (k + 2) * per_side

    def meet(r):
        if r > 0 and 2 ** (r - 1) < ns // 2:
            pl.semaphore_wait(met.at[r - 1], 2)
        if 2**r < ns // 2:
            for d in (2**r, -(2**r)):
                pl.semaphore_signal(
                    met.at[r], inc=1, device_id=(sp_at(d), t), device_id_type=MESH
                )

    def all_of(ref, sem):
        return pltpu.make_async_copy(ref, ref, sem)

    def send(src, dst, send_sem, recv_sem, device):
        copy = pltpu.make_async_remote_copy(
            src_ref=src,
            dst_ref=dst,
            send_sem=send_sem,
            recv_sem=recv_sem,
            device_id=device,
            device_id_type=MESH,
        )
        copy.start()
        return copy

    with jax.named_scope("signal"):
        barrier = pltpu.get_barrier_semaphore()
        for i in range(1, ntp):
            pl.semaphore_signal(
                barrier, inc=1, device_id=(s, lax.rem(t + i, ntp)), device_id_type=MESH
            )
        for d in (1, -1):
            pl.semaphore_signal(barrier, inc=1, device_id=(sp_at(d), t), device_id_type=MESH)

        loads = {}
        for i in (1, 2, 9, 3, 4, 5, 6, 8, 10, 0, 7, 11, 12, 13):
            source = sources[i].at[0] if i >= 11 else sources[i]
            loads[i] = pltpu.make_async_copy(source, scratch[i], load_sem.at[i])
        for load in loads.values():
            load.start()

    with jax.named_scope("local"):
        loads[1].wait()
        loads[2].wait()
        gated_f = value_ref[...].astype(F32) * jax.nn.sigmoid(gate_ref[...].astype(F32))
        gated[...] = gated_f.astype(BF16)
        padded[edge : edge + rows, :] = gated[...].astype(F32)

    with jax.named_scope("barrier"):
        pl.semaphore_wait(barrier, ntp - 1 + 2)
        meet(0)

    with jax.named_scope("halo"):
        for side, start, d in ((0, rows - edge, 1), (1, 0, -1)):
            send(
                gated.at[pl.ds(start, edge)],
                halo.at[side],
                halo_s.at[0],
                halo_r.at[0],
                (sp_at(d), t),
            )
        far_first = list(reversed(offsets[1:]))
        for i in (5, 6, 8):
            loads[i].wait()
        gains[t] = jnp.concatenate(
            [
                jnp.zeros((2, width), F32),
                1.0 / norm_gain_ref[...],
                ln_gain_ref[...],
                ln_bias_ref[...],
                jnp.zeros((3, width), F32),
            ],
            axis=0,
        )
        for o in far_first:
            send(gains.at[t], gains.at[t], stat_s.at[0], stat_r.at[0], (s, tp_at(*o)))
        meet(1)
        all_of(halo, halo_r.at[0]).wait()
        padded[0:edge, :] = jnp.where(s > 0, halo[0].astype(F32), 0.0)
        padded[edge + rows : edge + rows + edge, :] = jnp.where(
            s < ns - 1, halo[1].astype(F32), 0.0
        )
    with jax.named_scope("conv"):
        for i in (3, 4):
            loads[i].wait()
        tap_values = taps_ref[...].astype(F32)
        conv = jnp.zeros((rows, width), F32) + conv_bias_ref[...]
        for tap in range(taps):
            start = edge - reach + tap
            conv = conv + padded[start : start + rows, :] * tap_values[tap : tap + 1, :]
        conv_t = conv.T
        stat[t, 0:1, :] = jnp.sum(conv_t, axis=0, keepdims=True)
        stat[t, 1:2, :] = jnp.sum(conv_t * conv_t, axis=0, keepdims=True)
        sums_here = stat.at[t, pl.ds(0, 2)]
        for o in far_first:
            send(sums_here, sums_here, stat_s.at[1], stat_r.at[1], (s, tp_at(*o)))
        own_mean = jnp.sum(conv, axis=1, keepdims=True) * (1.0 / width)
        act[0] = (conv - own_mean).astype(BF16)
        half = ntp // 2
        for n, o in enumerate(far_first):
            sem = act_r.at[0 if n + 1 < half else 1]
            send(act.at[0], act.at[number[o]], act_s.at[0], sem, (s, tp_at(*o)))
    with jax.named_scope("route"):
        meet(2)
        for i in (9, 10, 0):
            loads[i].wait()
        expert_of = lax.broadcasted_iota(jnp.int32, (ns, rows), 0)
        chosen = [
            jnp.where(ids_ref[k : k + 1, :] == expert_of, 1.0, 0.0).astype(BF16)
            for k in range(TOPK)
        ]
        earlier = jnp.where(
            lax.broadcasted_iota(jnp.int32, (rows, rows), 0)
            < lax.broadcasted_iota(jnp.int32, (rows, rows), 1),
            1.0,
            0.0,
        ).astype(BF16)
        rank = jnp.dot(chosen[0] + chosen[1], earlier, preferred_element_type=F32).astype(BF16)
        slot = lax.broadcasted_iota(jnp.int32, (slots, ns), 0)
        in_chunk = (slot // cap) & (2 * per_side - 1)
        chunk_of = slot // depth_rows
        away = in_chunk + chunk_of * per_side
        away = jnp.where(in_chunk >= per_side, away - (2 * chunk_of + 2) * per_side, away)
        spread = jnp.where(
            lax.broadcasted_iota(jnp.int32, (slots, ns), 1) == ((s + away + 2 * ns) & (ns - 1)),
            1.0,
            0.0,
        ).astype(BF16)
        rank_at = jnp.dot(spread, rank, preferred_element_type=F32)
        slot_rank = (lax.broadcasted_iota(jnp.int32, (slots, rows), 0) & (cap - 1)).astype(F32)
        hit = rank_at == slot_rank
        both = jnp.zeros((slots, rows), F32)
        for k in range(TOPK):
            here = jnp.dot(spread, chosen[k], preferred_element_type=F32)
            here = jnp.where(hit, here, 0.0)
            picks[k] = here.T.astype(BF16)
            both = both + here
            route_cols[k] = jnp.broadcast_to(route_weight_ref[k : k + 1, :], (width, rows)).T
        places[...] = both.astype(BF16)
    with jax.named_scope("stats"):
        meet(3)
        all_of(gains.at[pl.ds(0, ntp - 1)], stat_r.at[0]).wait()
        all_of(stat.at[pl.ds(0, ntp - 1), pl.ds(0, 2)], stat_r.at[1]).wait()
        totals = jnp.sum(stat[:, 0:2, :], axis=0) * (1.0 / total_width)
        mean = totals[0:1, :]
        spread_inv = lax.rsqrt(totals[1:2, :] - mean * mean + 1e-05)
        lifts = [
            (stat[owner(o), 0:1, :] * (1.0 / width) - mean) * spread_inv for o in offsets
        ]
        lifts.append(spread_inv)
        lifts.append(jnp.zeros((rows - len(lifts), rows), F32))
        columns = jnp.concatenate(lifts, axis=0).T
        inv_col = columns[:, ntp : ntp + 1]
        total = residual_ref[...].astype(F32)
        loads[7].wait()
    with jax.named_scope("act_gather"):
        waiting = [(0, 0)] + far_first
        for n, group in enumerate((waiting[:half], waiting[half:])):
            blocks, tall = [], []
            if n == 1 or half > 1:
                all_of(act.at[pl.ds(0, half - 1 + n)], act_r.at[n]).wait()
            for o in group:
                i = number[o]
                who = owner(o)
                value = act[i].astype(F32) * inv_col + columns[:, i : i + 1]
                value = value * gains[who, 3:4, :] + gains[who, 4:5, :]
                blocks.append(jax.nn.silu(value).astype(BF16))
                tall.append(out_weight[pl.ds(pl.multiple_of(who * width, width), width), :])
            total = total + jnp.dot(
                jnp.concatenate(blocks, axis=1),
                jnp.concatenate(tall, axis=0),
                preferred_element_type=F32,
            )
    with jax.named_scope("project"):
        meet(4)
        mixed[...] = total
        scaled_rows = (total * norm_gain_ref[...]).astype(BF16)

    with jax.named_scope("dispatch"):
        outgoing[...] = jnp.dot(places[...], scaled_rows, preferred_element_type=F32).astype(BF16)
        for k in SEND_ORDER:
            for jj in range(2 * per_side):
                d = distance(k, jj)
                part, flat = pl.ds(jj * cap, cap), pl.ds(k * depth_rows + jj * cap, cap)
                if d == 0:
                    xbuf[k, 0, part, :] = outgoing[flat, :]
                else:
                    send(
                        outgoing.at[flat], xbuf.at[k, 0, part], z_s.at[0], z_r.at[k], (sp_at(d), t)
                    )
        for i in (11, 12, 13):
            loads[i].wait()

    def blocks_of(buffer, k, count):
        return buffer.at[k, pl.ds(0, count)]

    def arriving_leaves(k, index):
        tree = trees[k]
        return [o for o in tree.groups[index] if o != (0, 0) and not tree.children[o]]

    def pass_on(k, o):
        tree = trees[k]
        if o == (0, 0):
            here = cap if distance(k, 0) == 0 else 0
            all_of(xbuf.at[k, 0, pl.ds(0, depth_rows - here)], z_r.at[k]).wait()
        elif tree.children[o]:
            all_of(xbuf.at[k, number[o]], ag_r.at[k, tree.lane[o] - 1]).wait()
        for c in tree.children[o]:
            if tree.children[c]:
                sem = ag_r.at[k, tree.lane[c] - 1]
            else:
                sem = leaf_r.at[k, tree.group_of[c]]
            send(
                xbuf.at[k, number[o]],
                xbuf.at[k, number[c]],
                ag_s.at[0],
                sem,
                (s, tp_at(c[0] - o[0], c[1] - o[1])),
            )

    def multiply(k, index):
        group, first = trees[k].groups[index], index == 0
        leaves = arriving_leaves(k, index)
        if leaves:
            all_of(blocks_of(xbuf, k, len(leaves)), leaf_r.at[k, index]).wait()
        blocks = [xbuf[k, number[o]] for o in group]
        owners = [owner(o) for o in group]
        wide = jnp.concatenate(blocks, axis=1)
        squares = None if first else acc_sq[k]
        for block, who in zip(blocks, owners):
            plain = block.astype(F32) * gains[who, 2:3, :]
            squares = plain * plain if squares is None else squares + plain * plain
        acc_sq[k] = squares
        for weight, acc in ((expert_gate, acc_gate), (expert_up, acc_up)):
            tall = jnp.concatenate(
                [weight[pl.ds(pl.multiple_of(who * width, width), width), :] for who in owners],
                axis=0,
            )
            product = jnp.dot(wide, tall, preferred_element_type=F32)
            acc[k] = product if first else acc[k] + product

    def finish_rows(k):
        square = jnp.sum(acc_sq[k], axis=1, keepdims=True) * (1.0 / total_width)
        scale = lax.rsqrt(square + 1e-06)
        hidden = (jax.nn.silu(acc_gate[k] * scale) * (acc_up[k] * scale)).astype(BF16)
        for i in range(0, ntp, 2):
            pair = jnp.dot(
                hidden, expert_down[:, i * width : (i + 2) * width], preferred_element_type=F32
            ).astype(BF16)
            partial[k, i] = pair[:, :width]
            partial[k, i + 1] = pair[:, width:]

    def sum_up(k, o):
        who = owner(o)
        tree = trees[k]
        source = partial.at[k, who]
        if tree.children[o]:
            count = len(tree.children[o])
            all_of(blocks_of(rs_in, k, count), rs_r.at[k, tree.lane[o]]).wait()
            value = partial[k, who].astype(F32)
            for c in tree.children[o]:
                value = value + rs_in[k, number[c]].astype(F32)
            if o == (0, 0):
                ret_out[pl.ds(k * depth_rows, depth_rows), :] = value.astype(BF16)
                return
            rs_out[k, number[o]] = value.astype(BF16)
            source = rs_out.at[k, number[o]]
        p = tree.parent[o]
        send(
            source,
            rs_in.at[k, number[o]],
            rs_s.at[0],
            rs_r.at[k, tree.lane[p]],
            (s, tp_at(p[0] - o[0], p[1] - o[1])),
        )

    def give_back(k):
        for jj in range(2 * per_side):
            d = distance(k, jj)
            part = pl.ds(k * depth_rows + jj * cap, cap)
            if d == 0:
                ret_in[part, :] = ret_out[part, :]
            else:
                send(ret_out.at[part], ret_in.at[part], rt_s.at[0], rt_r.at[0], (sp_at(-d), t))

    along = [5.6 * (2 * k + 1) / chunks**2 for k in range(chunks)]
    arrivals, clock = {}, 0.0
    for k in SEND_ORDER:
        clock += along[k]
        arrivals[k] = clock + 1.7 + 0.8 * (8 / chunks) * (k + 1)
    for kind, k, o in plan(trees, nx, ny, depth_rows, arrivals, URGENCY, SUM_URGENCY, LEAD):
        with jax.named_scope(f"{kind}{k}{o}"):
            if kind == "pass":
                pass_on(k, o)
            elif kind == "multiply":
                multiply(k, o)
            elif kind == "finish":
                finish_rows(k)
            else:
                sum_up(k, o)
                if o == (0, 0):
                    give_back(k)
    away_rows = pl.ds(0, slots - cap)
    with jax.named_scope("wait_sends"):
        all_of(halo, halo_s.at[0]).wait()
        all_of(gains.at[pl.ds(0, ntp - 1)], stat_s.at[0]).wait()
        all_of(stat.at[pl.ds(0, ntp - 1), pl.ds(0, 2)], stat_s.at[1]).wait()
        all_of(act.at[pl.ds(0, ntp - 1)], act_s.at[0]).wait()
        all_of(outgoing.at[away_rows], z_s.at[0]).wait()
        all_of(xbuf.at[:, pl.ds(0, ntp - 1)], ag_s.at[0]).wait()
        all_of(rs_in.at[:, pl.ds(0, ntp - 1)], rs_s.at[0]).wait()
    with jax.named_scope("wait_back"):
        all_of(ret_in.at[away_rows], rt_r.at[0]).wait()
    with jax.named_scope("result"):
        answer = ret_in[...]
        result = mixed[...]
        for k in range(TOPK):
            picked = jnp.dot(picks[k], answer, preferred_element_type=F32)
            result = result + picked * route_cols[k]
        out_ref[...] = result.astype(BF16)

    with jax.named_scope("end"):
        all_of(ret_out.at[away_rows], rt_s.at[0]).wait()


def on_device(ns, nx, ny, *args):
    (
        residual,
        glu_value,
        glu_gate,
        conv_weight,
        conv_bias,
        ln_gain,
        ln_bias,
        out_weight,
        norm_gain,
        route_ids,
        route_weight,
        expert_gate,
        expert_up,
        expert_down,
    ) = args
    ntp = nx * ny
    rows, width = residual.shape
    hidden = expert_gate.shape[2]
    capacity = 2 * rows * TOPK // ns
    slots = ns * capacity
    k, rc = CHUNKS, slots // CHUNKS
    edge = 16
    row = lambda v: v.reshape(1, -1)
    vmem = pl.BlockSpec(memory_space=pltpu.VMEM)
    hbm = pl.BlockSpec(memory_space=pltpu.HBM)
    dma = pltpu.SemaphoreType.DMA
    operands = (
        residual,
        glu_value,
        glu_gate,
        conv_weight,
        row(conv_bias),
        row(ln_gain),
        row(ln_bias),
        out_weight,
        row(norm_gain),
        route_ids.T,
        route_weight.T,
        expert_gate,
        expert_up,
        expert_down,
    )
    return pl.pallas_call(
        functools.partial(layer_kernel, ns, nx, ny),
        out_shape=jax.ShapeDtypeStruct(residual.shape, BF16),
        in_specs=[hbm] * 14,
        out_specs=vmem,
        scratch_shapes=[
            *[pltpu.VMEM(a.shape[-2:], a.dtype) for a in operands],
            pltpu.VMEM((2, edge, width), BF16),
            pltpu.VMEM((rows, width), BF16),
            pltpu.VMEM((rows + 2 * edge, width), F32),
            pltpu.VMEM((ntp, 8, width), F32),
            pltpu.VMEM((ntp, 8, width), F32),
            pltpu.VMEM((ntp, rows, width), BF16),
            pltpu.VMEM((rows, width), F32),
            pltpu.VMEM((TOPK, rows, slots), BF16),
            pltpu.VMEM((slots, rows), BF16),
            pltpu.VMEM((TOPK, rows, width), F32),
            pltpu.VMEM((slots, width), BF16),
            pltpu.VMEM((k, ntp, rc, width), BF16),
            pltpu.VMEM((k, rc, hidden), F32),
            pltpu.VMEM((k, rc, hidden), F32),
            pltpu.VMEM((k, rc, width), F32),
            pltpu.VMEM((k, ntp, rc, width), BF16),
            pltpu.VMEM((k, ntp, rc, width), BF16),
            pltpu.VMEM((k, ntp, rc, width), BF16),
            pltpu.VMEM((slots, width), BF16),
            pltpu.VMEM((slots, width), BF16),
            pltpu.SemaphoreType.REGULAR((4,)),
            dma((14,)),
            dma((1,)),
            dma((1,)),
            dma((2,)),
            dma((2,)),
            dma((1,)),
            dma((2,)),
            dma((1,)),
            dma((k,)),
            dma((1,)),
            dma((k, 9)),
            dma((k, 3)),
            dma((1,)),
            dma((k, 10)),
            dma((1,)),
            dma((1,)),
        ],
        compiler_params=pltpu.CompilerParams(
            collective_id=0, has_side_effects=True, vmem_limit_bytes=66 * 1000 * 1000
        ),
        name="layer",
    )(*operands)


IN_SPECS = (
    P("sp", "tp"),
    P("sp", "tp"),
    P("sp", "tp"),
    P(None, "tp"),
    P("tp"),
    P("tp"),
    P("tp"),
    P(None, "tp"),
    P("tp"),
    P("sp", None),
    P("sp", None),
    P("sp", None, "tp"),
    P("sp", None, "tp"),
    P("sp", "tp", None),
)


def solution(mesh, nx=NX):
    ns, ntp = mesh.shape["sp"], mesh.shape["tp"]
    return jax.shard_map(
        functools.partial(on_device, ns, nx, ntp // nx),
        mesh=mesh,
        in_specs=IN_SPECS,
        out_specs=P("sp", "tp"),
        check_vma=False,
    )
```

```python
import functools

import jax
import jax.numpy as jnp
from jax import lax
from jax.experimental import pallas as pl
from jax.experimental.pallas import tpu as pltpu
from jax.sharding import PartitionSpec as P

MESH = pl.DeviceIdType.MESH
TOPK = 2
F32 = jnp.float32
BF16 = jnp.bfloat16
NX = 4
CHUNKS = 8
SEND_ORDER = (0, 2, 7, 3, 1, 6, 4, 5)
URGENCY = (2, 6, 7, 5, 4, 3, 1, 0)
SUM_URGENCY = (4, 5, 3, 6, 7, 1, 0, 2)
KINDS = (1, 1, 1, 1, 1, 1, 1, 1)
LEAD = 0.7

TREE_4X4 = {
    (1, 0): (0, 0),
    (3, 0): (0, 0),
    (0, 1): (0, 0),
    (0, 3): (0, 0),
    (1, 1): (1, 0),
    (3, 1): (0, 1),
    (3, 3): (3, 0),
    (1, 3): (0, 3),
    (2, 0): (1, 0),
    (0, 2): (0, 3),
    (2, 1): (3, 1),
    (2, 3): (1, 3),
    (1, 2): (1, 1),
    (3, 2): (3, 3),
    (2, 2): (2, 1),
}
SHALLOW_4X4 = {
    **{o: (0, 0) for o in TREE_4X4},
    (2, 0): (1, 0),
    (0, 2): (0, 3),
    (2, 1): (1, 1),
    (2, 3): (3, 3),
    (1, 2): (1, 3),
    (3, 2): (3, 1),
    (2, 2): (1, 1),
}
DIRECT_4X4 = {o: (0, 0) for o in TREE_4X4}


def turned(tree, quarters):
    def turn(o):
        for _ in range(quarters):
            o = (-o[1] % 4, o[0])
        return o

    return {turn(c): turn(p) for c, p in tree.items()}


class Tree:
    def __init__(self, nx, ny, kind, quarters):
        if (nx, ny) == (4, 4):
            parent = turned((TREE_4X4, SHALLOW_4X4, DIRECT_4X4)[kind], quarters)
        else:
            parent, frontier = {}, [(0, 0)]
            while frontier:
                grown = []
                for px, py in frontier:
                    for dx, dy in ((1, 0), (nx - 1, 0), (0, 1), (0, ny - 1)):
                        o = ((px + dx) % nx, (py + dy) % ny)
                        if o != (0, 0) and o not in parent:
                            parent[o] = (px, py)
                            grown.append(o)
                frontier = grown
        self.parent = parent
        self.depth = {(0, 0): 0}
        self.order = [(0, 0)]
        for o in self.order:
            for c in sorted(parent):
                if parent[c] == o:
                    self.depth[c] = self.depth[o] + 1
                    self.order.append(c)
        self.children = {o: [c for c in self.order if parent.get(c) == o] for o in self.order}
        self.groups = [
            [o for o in self.order if low <= self.depth[o] <= high]
            for low, high in ((0, 1), (2, 2), (3, 9))
        ]
        self.groups = [g for g in self.groups if g]
        relays = [o for o in self.order if self.children[o]]
        leaf_groups = [
            i for i, g in enumerate(self.groups) if any(not self.children[o] for o in g)
        ]
        group_of = {o: i for i, g in enumerate(self.groups) for o in g}
        self.lane = {o: i - 1 for i, o in enumerate(relays)}
        for o in self.order:
            if o not in self.lane:
                self.lane[o] = len(relays) - 1 + leaf_groups.index(group_of[o])
        self.lanes = len(relays) - 1 + len(leaf_groups)
        self.sum_lane = {o: i for i, o in enumerate(relays)}
        self.sum_lanes = len(relays)


def chunk_trees(nx, ny):
    return [Tree(nx, ny, KINDS[k], k) for k in range(CHUNKS)]


def signed(v, n):
    return (v + n // 2 - 1) % n - (n // 2 - 1)


def plan(trees, nx, ny, rows, arrivals, urgency, sum_urgency, lead):
    wire, latency, hop = rows * 256 / 46.65e3, 2.6, 0.75
    link, now, steps, pending = {}, 0.0, [], []
    arrived, summed, passed, given = {}, {}, {}, {}

    def sent(p, o):
        dx, dy = signed(o[0] - p[0], nx), signed(o[1] - p[1], ny)
        end = now
        for axis, v, n in ((0, dx, nx), (1, dy, ny)):
            if v:
                for way in (1, -1) if 2 * v == n else (1 if v > 0 else -1,):
                    link[axis, way] = max(link.get((axis, way), 0.0), now) + wire
                    end = max(end, link[axis, way])
        return end + latency + hop * (abs(dx) + abs(dy) - 1)

    def way(p, o):
        dx, dy = signed(o[0] - p[0], nx), signed(o[1] - p[1], ny)
        return (0, 1 if dx > 0 else -1) if dx else (1, 1 if dy > 0 else -1)

    for k in range(len(trees)):
        pending.append(("pass", k, (0, 0)))
        passed[k], given[k] = set(), 0
    finished = 0
    while finished < len(trees):
        ready = {}
        for e in pending:
            kind, k, o = e
            if kind == "pass":
                ready[e] = arrived[k, o] if o != (0, 0) else arrivals[k]
                ways = [way(o, c) for c in trees[k].children[o]]
            elif kind == "sum":
                ready[e] = max([summed[k, c] for c in trees[k].children[o]], default=0.0)
                ways = [way(o, trees[k].parent[o])] if o != (0, 0) else []
            else:
                ready[e] = 0.0
                ways = []
            if ways:
                ready[e] = max(ready[e], min(link.get(w, 0.0) for w in ways) - lead)

        def rank(e):
            kind, k, o = e
            late = -trees[k].depth[o] if kind == "sum" else 0
            first = (sum_urgency if kind == "sum" else urgency)[k]
            return ({"pass": 0, "sum": 0, "finish": 1}.get(kind, 2), first, late, str(o))

        able = [e for e in pending if ready[e] <= now + 1e-9]
        if able:
            e = min(able, key=rank)
        else:
            e = min(pending, key=lambda e: (ready[e], rank(e)))
        pending.remove(e)
        now = max(now, ready[e])
        steps.append(e)
        kind, k, o = e
        tree = trees[k]
        if kind == "pass":
            for c in tree.children[o]:
                arrived[k, c] = sent(o, c)
                pending.append(("pass", k, c))
            now += 0.04
            passed[k].add(o)
            while given[k] < len(tree.groups) and passed[k].issuperset(tree.groups[given[k]]):
                pending.append(("multiply", k, given[k]))
                given[k] += 1
        elif kind == "multiply":
            now += 0.15
            if given[k] == len(tree.groups) and not any(e[:2] == (kind, k) for e in pending):
                pending.append(("finish", k, 0))
        elif kind == "finish":
            now += 0.38
            pending += [("sum", k, c) for c in tree.order if not tree.children[c]]
        else:
            now += 0.05 if tree.children[o] else 0.02
            if o == (0, 0):
                finished += 1
            else:
                p = tree.parent[o]
                summed[k, o] = sent(o, p)
                if all((k, c) in summed for c in tree.children[p]):
                    pending.append(("sum", k, p))
    return steps


def layer_kernel(
    ns,
    nx,
    ny,
    *refs,
):
    sources, (out_ref, *scratch) = refs[:14], refs[14:]
    (
        residual_ref,
        value_ref,
        gate_ref,
        taps_ref,
        conv_bias_ref,
        ln_gain_ref,
        ln_bias_ref,
        out_weight,
        norm_gain_ref,
        ids_ref,
        route_weight_ref,
        expert_gate,
        expert_up,
        expert_down,
    ) = scratch[:14]
    (
        halo,
        gated,
        padded,
        stat,
        gains,
        act,
        mixed,
        picks,
        places,
        route_cols,
        outgoing,
        xbuf,
        acc_gate,
        acc_up,
        acc_sq,
        partial,
        rs_in,
        rs_out,
        ret_out,
        ret_in,
        met,
        load_sem,
        halo_s,
        halo_r,
        stat_s,
        stat_r,
        act_s,
        act_r,
        z_s,
        z_r,
        ag_s,
        ag_r,
        rs_s,
        rs_r,
        rt_s,
        rt_r,
    ) = scratch[14:]
    ntp = nx * ny
    rows, width = residual_ref.shape
    total_width = ntp * width
    slots = places.shape[0]
    cap = slots // ns
    chunks = xbuf.shape[0]
    depth_rows = slots // chunks
    per_side = ns // (2 * chunks)
    taps = taps_ref.shape[0]
    reach = taps // 2
    edge = halo.shape[1]
    s = lax.axis_index("sp")
    t = lax.axis_index("tp")
    ty, tx = t // nx, lax.rem(t, nx)
    trees = chunk_trees(nx, ny)
    ag_base = [sum(tree.lanes for tree in trees[:k]) for k in range(chunks)]
    rs_base = [sum(tree.sum_lanes for tree in trees[:k]) for k in range(chunks)]
    offsets = sorted(trees[0].order, key=lambda o: (abs(signed(o[0], nx)) + abs(signed(o[1], ny)), o))
    number = {o: i for i, o in enumerate(offsets)}

    def tp_at(dx, dy):
        return lax.rem(ty + dy + 2 * ny, ny) * nx + lax.rem(tx + dx + 2 * nx, nx)

    def owner(o):
        return tp_at(-o[0], -o[1])

    def sp_at(d):
        return lax.rem(s + d + 2 * ns, ns)

    def distance(k, jj):
        return k * per_side + jj if jj < per_side else jj - (k + 2) * per_side

    def meet(r):
        if r > 0 and 2 ** (r - 1) < ns // 2:
            pl.semaphore_wait(met.at[r - 1], 2)
        if 2**r < ns // 2:
            for d in (2**r, -(2**r)):
                pl.semaphore_signal(
                    met.at[r], inc=1, device_id=(sp_at(d), t), device_id_type=MESH
                )

    def all_of(ref, sem):
        return pltpu.make_async_copy(ref, ref, sem)

    def send(src, dst, send_sem, recv_sem, device):
        copy = pltpu.make_async_remote_copy(
            src_ref=src,
            dst_ref=dst,
            send_sem=send_sem,
            recv_sem=recv_sem,
            device_id=device,
            device_id_type=MESH,
        )
        copy.start()
        return copy

    with jax.named_scope("signal"):
        barrier = pltpu.get_barrier_semaphore()
        for i in range(1, ntp):
            pl.semaphore_signal(
                barrier, inc=1, device_id=(s, lax.rem(t + i, ntp)), device_id_type=MESH
            )
        for d in (1, -1):
            pl.semaphore_signal(barrier, inc=1, device_id=(sp_at(d), t), device_id_type=MESH)

        loads = {}
        for i in (1, 2, 9, 3, 4, 5, 6, 8, 10, 0, 7, 11, 12, 13):
            source = sources[i].at[0] if i >= 11 else sources[i]
            loads[i] = pltpu.make_async_copy(source, scratch[i], load_sem.at[i])
        for load in loads.values():
            load.start()

    with jax.named_scope("local"):
        loads[1].wait()
        loads[2].wait()
        gated_f = value_ref[...].astype(F32) * jax.nn.sigmoid(gate_ref[...].astype(F32))
        gated[...] = gated_f.astype(BF16)
        padded[edge : edge + rows, :] = gated[...].astype(F32)

    with jax.named_scope("barrier"):
        pl.semaphore_wait(barrier, ntp - 1 + 2)
        meet(0)

    with jax.named_scope("halo"):
        for side, start, d in ((0, rows - edge, 1), (1, 0, -1)):
            send(
                gated.at[pl.ds(start, edge)],
                halo.at[side],
                halo_s.at[0],
                halo_r.at[0],
                (sp_at(d), t),
            )
        far_first = list(reversed(offsets[1:]))
        for i in (5, 6, 8):
            loads[i].wait()
        gains[t] = jnp.concatenate(
            [
                jnp.zeros((2, width), F32),
                1.0 / norm_gain_ref[...],
                ln_gain_ref[...],
                ln_bias_ref[...],
                jnp.zeros((3, width), F32),
            ],
            axis=0,
        )
        for o in far_first:
            send(gains.at[t], gains.at[t], stat_s.at[0], stat_r.at[0], (s, tp_at(*o)))
        meet(1)
        all_of(halo, halo_r.at[0]).wait()
        padded[0:edge, :] = jnp.where(s > 0, halo[0].astype(F32), 0.0)
        padded[edge + rows : edge + rows + edge, :] = jnp.where(
            s < ns - 1, halo[1].astype(F32), 0.0
        )
    with jax.named_scope("conv"):
        for i in (3, 4):
            loads[i].wait()
        tap_values = taps_ref[...].astype(F32)
        conv = jnp.zeros((rows, width), F32) + conv_bias_ref[...]
        for tap in range(taps):
            start = edge - reach + tap
            conv = conv + padded[start : start + rows, :] * tap_values[tap : tap + 1, :]
        conv_t = conv.T
        stat[t, 0:1, :] = jnp.sum(conv_t, axis=0, keepdims=True)
        stat[t, 1:2, :] = jnp.sum(conv_t * conv_t, axis=0, keepdims=True)
        sums_here = stat.at[t, pl.ds(0, 2)]
        for o in far_first:
            send(sums_here, sums_here, stat_s.at[1], stat_r.at[1], (s, tp_at(*o)))
        own_mean = jnp.sum(conv, axis=1, keepdims=True) * (1.0 / width)
        act[0] = (conv - own_mean).astype(BF16)
        half = ntp // 2
        for n, o in enumerate(far_first):
            sem = act_r.at[0 if n + 1 < half else 1]
            send(act.at[0], act.at[number[o]], act_s.at[0], sem, (s, tp_at(*o)))
    with jax.named_scope("route"):
        meet(2)
        for i in (9, 10, 0):
            loads[i].wait()
        expert_of = lax.broadcasted_iota(jnp.int32, (ns, rows), 0)
        chosen = [
            jnp.where(ids_ref[k : k + 1, :] == expert_of, 1.0, 0.0).astype(BF16)
            for k in range(TOPK)
        ]
        earlier = jnp.where(
            lax.broadcasted_iota(jnp.int32, (rows, rows), 0)
            < lax.broadcasted_iota(jnp.int32, (rows, rows), 1),
            1.0,
            0.0,
        ).astype(BF16)
        rank = jnp.dot(chosen[0] + chosen[1], earlier, preferred_element_type=F32).astype(BF16)
        slot = lax.broadcasted_iota(jnp.int32, (slots, ns), 0)
        in_chunk = (slot // cap) & (2 * per_side - 1)
        chunk_of = slot // depth_rows
        away = in_chunk + chunk_of * per_side
        away = jnp.where(in_chunk >= per_side, away - (2 * chunk_of + 2) * per_side, away)
        spread = jnp.where(
            lax.broadcasted_iota(jnp.int32, (slots, ns), 1) == ((s + away + 2 * ns) & (ns - 1)),
            1.0,
            0.0,
        ).astype(BF16)
        rank_at = jnp.dot(spread, rank, preferred_element_type=F32)
        slot_rank = (lax.broadcasted_iota(jnp.int32, (slots, rows), 0) & (cap - 1)).astype(F32)
        hit = rank_at == slot_rank
        both = jnp.zeros((slots, rows), F32)
        for k in range(TOPK):
            here = jnp.dot(spread, chosen[k], preferred_element_type=F32)
            here = jnp.where(hit, here, 0.0)
            picks[k] = here.T.astype(BF16)
            both = both + here
            route_cols[k] = jnp.broadcast_to(route_weight_ref[k : k + 1, :], (width, rows)).T
        places[...] = both.astype(BF16)
    with jax.named_scope("stats"):
        meet(3)
        all_of(gains.at[pl.ds(0, ntp - 1)], stat_r.at[0]).wait()
        all_of(stat.at[pl.ds(0, ntp - 1), pl.ds(0, 2)], stat_r.at[1]).wait()
        totals = jnp.sum(stat[:, 0:2, :], axis=0) * (1.0 / total_width)
        mean = totals[0:1, :]
        spread_inv = lax.rsqrt(totals[1:2, :] - mean * mean + 1e-05)
        lifts = [
            (stat[owner(o), 0:1, :] * (1.0 / width) - mean) * spread_inv for o in offsets
        ]
        lifts.append(spread_inv)
        lifts.append(jnp.zeros((rows - len(lifts), rows), F32))
        columns = jnp.concatenate(lifts, axis=0).T
        inv_col = columns[:, ntp : ntp + 1]
        total = residual_ref[...].astype(F32)
        loads[7].wait()
    with jax.named_scope("act_gather"):
        waiting = [(0, 0)] + far_first
        for n, group in enumerate((waiting[:half], waiting[half:])):
            blocks, tall = [], []
            if n == 1 or half > 1:
                all_of(act.at[pl.ds(0, half - 1 + n)], act_r.at[n]).wait()
            for o in group:
                i = number[o]
                who = owner(o)
                value = act[i].astype(F32) * inv_col + columns[:, i : i + 1]
                value = value * gains[who, 3:4, :] + gains[who, 4:5, :]
                blocks.append(jax.nn.silu(value).astype(BF16))
                tall.append(out_weight[pl.ds(pl.multiple_of(who * width, width), width), :])
            total = total + jnp.dot(
                jnp.concatenate(blocks, axis=1),
                jnp.concatenate(tall, axis=0),
                preferred_element_type=F32,
            )
    with jax.named_scope("project"):
        meet(4)
        mixed[...] = total
        scaled_rows = (total * norm_gain_ref[...]).astype(BF16)

    with jax.named_scope("dispatch"):
        outgoing[...] = jnp.dot(places[...], scaled_rows, preferred_element_type=F32).astype(BF16)
        for k in SEND_ORDER:
            for jj in range(2 * per_side):
                d = distance(k, jj)
                part, flat = pl.ds(jj * cap, cap), pl.ds(k * depth_rows + jj * cap, cap)
                if d == 0:
                    xbuf[k, 0, part, :] = outgoing[flat, :]
                else:
                    send(
                        outgoing.at[flat], xbuf.at[k, 0, part], z_s.at[0], z_r.at[k], (sp_at(d), t)
                    )
        for i in (11, 12, 13):
            loads[i].wait()

    def blocks_of(buffer, k, count):
        return buffer.at[k, pl.ds(0, count)]

    def arriving_leaves(k, index):
        tree = trees[k]
        return [o for o in tree.groups[index] if o != (0, 0) and not tree.children[o]]

    def pass_on(k, o):
        tree = trees[k]
        if o == (0, 0):
            here = cap if distance(k, 0) == 0 else 0
            all_of(xbuf.at[k, 0, pl.ds(0, depth_rows - here)], z_r.at[k]).wait()
        elif tree.children[o]:
            all_of(xbuf.at[k, number[o]], ag_r.at[ag_base[k] + tree.lane[o]]).wait()
        for c in tree.children[o]:
            sem = ag_r.at[ag_base[k] + tree.lane[c]]
            send(
                xbuf.at[k, number[o]],
                xbuf.at[k, number[c]],
                ag_s.at[0],
                sem,
                (s, tp_at(c[0] - o[0], c[1] - o[1])),
            )

    def multiply(k, index):
        group, first = trees[k].groups[index], index == 0
        leaves = arriving_leaves(k, index)
        if leaves:
            sem = ag_r.at[ag_base[k] + trees[k].lane[leaves[0]]]
            all_of(blocks_of(xbuf, k, len(leaves)), sem).wait()
        blocks = [xbuf[k, number[o]] for o in group]
        owners = [owner(o) for o in group]
        wide = jnp.concatenate(blocks, axis=1)
        squares = None if first else acc_sq[k]
        for block, who in zip(blocks, owners):
            plain = block.astype(F32) * gains[who, 2:3, :]
            squares = plain * plain if squares is None else squares + plain * plain
        acc_sq[k] = squares
        for weight, acc in ((expert_gate, acc_gate), (expert_up, acc_up)):
            tall = jnp.concatenate(
                [weight[pl.ds(pl.multiple_of(who * width, width), width), :] for who in owners],
                axis=0,
            )
            product = jnp.dot(wide, tall, preferred_element_type=F32)
            acc[k] = product if first else acc[k] + product

    def finish_rows(k):
        square = jnp.sum(acc_sq[k], axis=1, keepdims=True) * (1.0 / total_width)
        scale = lax.rsqrt(square + 1e-06)
        hidden = (jax.nn.silu(acc_gate[k] * scale) * (acc_up[k] * scale)).astype(BF16)
        for i in range(0, ntp, 2):
            pair = jnp.dot(
                hidden, expert_down[:, i * width : (i + 2) * width], preferred_element_type=F32
            ).astype(BF16)
            partial[k, i] = pair[:, :width]
            partial[k, i + 1] = pair[:, width:]

    def sum_up(k, o):
        who = owner(o)
        tree = trees[k]
        source = partial.at[k, who]
        if tree.children[o]:
            count = len(tree.children[o])
            all_of(blocks_of(rs_in, k, count), rs_r.at[rs_base[k] + tree.sum_lane[o]]).wait()
            value = partial[k, who].astype(F32)
            for c in tree.children[o]:
                value = value + rs_in[k, number[c]].astype(F32)
            if o == (0, 0):
                ret_out[pl.ds(k * depth_rows, depth_rows), :] = value.astype(BF16)
                return
            rs_out[k, number[o]] = value.astype(BF16)
            source = rs_out.at[k, number[o]]
        p = tree.parent[o]
        send(
            source,
            rs_in.at[k, number[o]],
            rs_s.at[0],
            rs_r.at[rs_base[k] + tree.sum_lane[p]],
            (s, tp_at(p[0] - o[0], p[1] - o[1])),
        )

    def give_back(k):
        for jj in range(2 * per_side):
            d = distance(k, jj)
            part = pl.ds(k * depth_rows + jj * cap, cap)
            if d == 0:
                ret_in[part, :] = ret_out[part, :]
            else:
                send(ret_out.at[part], ret_in.at[part], rt_s.at[0], rt_r.at[0], (sp_at(-d), t))

    along = [5.6 * (2 * k + 1) / chunks**2 for k in range(chunks)]
    arrivals, clock = {}, 0.0
    for k in SEND_ORDER:
        clock += along[k]
        arrivals[k] = clock + 1.7 + 0.8 * (8 / chunks) * (k + 1)
    for kind, k, o in plan(trees, nx, ny, depth_rows, arrivals, URGENCY, SUM_URGENCY, LEAD):
        with jax.named_scope(f"{kind}{k}{o}"):
            if kind == "pass":
                pass_on(k, o)
            elif kind == "multiply":
                multiply(k, o)
            elif kind == "finish":
                finish_rows(k)
            else:
                sum_up(k, o)
                if o == (0, 0):
                    give_back(k)
    away_rows = pl.ds(0, slots - cap)
    with jax.named_scope("wait_sends"):
        all_of(halo, halo_s.at[0]).wait()
        all_of(gains.at[pl.ds(0, ntp - 1)], stat_s.at[0]).wait()
        all_of(stat.at[pl.ds(0, ntp - 1), pl.ds(0, 2)], stat_s.at[1]).wait()
        all_of(act.at[pl.ds(0, ntp - 1)], act_s.at[0]).wait()
        all_of(outgoing.at[away_rows], z_s.at[0]).wait()
        all_of(xbuf.at[:, pl.ds(0, ntp - 1)], ag_s.at[0]).wait()
        all_of(rs_in.at[:, pl.ds(0, ntp - 1)], rs_s.at[0]).wait()
    with jax.named_scope("wait_back"):
        all_of(ret_in.at[away_rows], rt_r.at[0]).wait()
    with jax.named_scope("result"):
        answer = ret_in[...]
        result = mixed[...]
        for k in range(TOPK):
            picked = jnp.dot(picks[k], answer, preferred_element_type=F32)
            result = result + picked * route_cols[k]
        out_ref[...] = result.astype(BF16)

    with jax.named_scope("end"):
        all_of(ret_out.at[away_rows], rt_s.at[0]).wait()


def on_device(ns, nx, ny, *args):
    (
        residual,
        glu_value,
        glu_gate,
        conv_weight,
        conv_bias,
        ln_gain,
        ln_bias,
        out_weight,
        norm_gain,
        route_ids,
        route_weight,
        expert_gate,
        expert_up,
        expert_down,
    ) = args
    ntp = nx * ny
    rows, width = residual.shape
    hidden = expert_gate.shape[2]
    capacity = 2 * rows * TOPK // ns
    slots = ns * capacity
    k, rc = CHUNKS, slots // CHUNKS
    edge = 16
    row = lambda v: v.reshape(1, -1)
    vmem = pl.BlockSpec(memory_space=pltpu.VMEM)
    hbm = pl.BlockSpec(memory_space=pltpu.HBM)
    dma = pltpu.SemaphoreType.DMA
    operands = (
        residual,
        glu_value,
        glu_gate,
        conv_weight,
        row(conv_bias),
        row(ln_gain),
        row(ln_bias),
        out_weight,
        row(norm_gain),
        route_ids.T,
        route_weight.T,
        expert_gate,
        expert_up,
        expert_down,
    )
    return pl.pallas_call(
        functools.partial(layer_kernel, ns, nx, ny),
        out_shape=jax.ShapeDtypeStruct(residual.shape, BF16),
        in_specs=[hbm] * 14,
        out_specs=vmem,
        scratch_shapes=[
            *[pltpu.VMEM(a.shape[-2:], a.dtype) for a in operands],
            pltpu.VMEM((2, edge, width), BF16),
            pltpu.VMEM((rows, width), BF16),
            pltpu.VMEM((rows + 2 * edge, width), F32),
            pltpu.VMEM((ntp, 8, width), F32),
            pltpu.VMEM((ntp, 8, width), F32),
            pltpu.VMEM((ntp, rows, width), BF16),
            pltpu.VMEM((rows, width), F32),
            pltpu.VMEM((TOPK, rows, slots), BF16),
            pltpu.VMEM((slots, rows), BF16),
            pltpu.VMEM((TOPK, rows, width), F32),
            pltpu.VMEM((slots, width), BF16),
            pltpu.VMEM((k, ntp, rc, width), BF16),
            pltpu.VMEM((k, rc, hidden), F32),
            pltpu.VMEM((k, rc, hidden), F32),
            pltpu.VMEM((k, rc, width), F32),
            pltpu.VMEM((k, ntp, rc, width), BF16),
            pltpu.VMEM((k, ntp, rc, width), BF16),
            pltpu.VMEM((k, ntp, rc, width), BF16),
            pltpu.VMEM((slots, width), BF16),
            pltpu.VMEM((slots, width), BF16),
            pltpu.SemaphoreType.REGULAR((4,)),
            dma((14,)),
            dma((1,)),
            dma((1,)),
            dma((2,)),
            dma((2,)),
            dma((1,)),
            dma((2,)),
            dma((1,)),
            dma((k,)),
            dma((1,)),
            dma((sum(tree.lanes for tree in chunk_trees(nx, ny)),)),
            dma((1,)),
            dma((sum(tree.sum_lanes for tree in chunk_trees(nx, ny)),)),
            dma((1,)),
            dma((1,)),
        ],
        compiler_params=pltpu.CompilerParams(
            collective_id=0, has_side_effects=True, vmem_limit_bytes=66 * 1000 * 1000
        ),
        name="layer",
    )(*operands)


IN_SPECS = (
    P("sp", "tp"),
    P("sp", "tp"),
    P("sp", "tp"),
    P(None, "tp"),
    P("tp"),
    P("tp"),
    P("tp"),
    P(None, "tp"),
    P("tp"),
    P("sp", None),
    P("sp", None),
    P("sp", None, "tp"),
    P("sp", None, "tp"),
    P("sp", "tp", None),
)


def solution(mesh, nx=NX):
    ns, ntp = mesh.shape["sp"], mesh.shape["tp"]
    return jax.shard_map(
        functools.partial(on_device, ns, nx, ntp // nx),
        mesh=mesh,
        in_specs=IN_SPECS,
        out_specs=P("sp", "tp"),
        check_vma=False,
    )
```

```python
import functools

import jax
import jax.numpy as jnp
from jax import lax
from jax.experimental import pallas as pl
from jax.experimental.pallas import tpu as pltpu
from jax.sharding import PartitionSpec as P

MESH = pl.DeviceIdType.MESH
TOPK = 2
F32 = jnp.float32
BF16 = jnp.bfloat16
NX = 4
CHUNKS = 8
SEND_ORDER = (1, 7, 4, 0, 2, 3, 6, 5)
URGENCY = (6, 0, 3, 7, 4, 2, 1, 5)
SUM_URGENCY = (5, 7, 6, 1, 4, 3, 2, 0)
KINDS = (1, 1, 1, 1, 1, 1, 1, 1)
LEAD = 0.3

TREE_4X4 = {
    (1, 0): (0, 0),
    (3, 0): (0, 0),
    (0, 1): (0, 0),
    (0, 3): (0, 0),
    (1, 1): (1, 0),
    (3, 1): (0, 1),
    (3, 3): (3, 0),
    (1, 3): (0, 3),
    (2, 0): (1, 0),
    (0, 2): (0, 3),
    (2, 1): (3, 1),
    (2, 3): (1, 3),
    (1, 2): (1, 1),
    (3, 2): (3, 3),
    (2, 2): (2, 1),
}
SHALLOW_4X4 = {
    **{o: (0, 0) for o in TREE_4X4},
    (2, 0): (1, 0),
    (0, 2): (0, 3),
    (2, 1): (1, 1),
    (2, 3): (3, 3),
    (1, 2): (1, 3),
    (3, 2): (3, 1),
    (2, 2): (1, 1),
}
DIRECT_4X4 = {o: (0, 0) for o in TREE_4X4}


def turned(tree, quarters):
    def turn(o):
        for _ in range(quarters):
            o = (-o[1] % 4, o[0])
        return o

    return {turn(c): turn(p) for c, p in tree.items()}


class Tree:
    def __init__(self, nx, ny, kind, quarters):
        if (nx, ny) == (4, 4):
            parent = turned((TREE_4X4, SHALLOW_4X4, DIRECT_4X4)[kind], quarters)
        else:
            parent, frontier = {}, [(0, 0)]
            while frontier:
                grown = []
                for px, py in frontier:
                    for dx, dy in ((1, 0), (nx - 1, 0), (0, 1), (0, ny - 1)):
                        o = ((px + dx) % nx, (py + dy) % ny)
                        if o != (0, 0) and o not in parent:
                            parent[o] = (px, py)
                            grown.append(o)
                frontier = grown
        self.parent = parent
        self.depth = {(0, 0): 0}
        self.order = [(0, 0)]
        for o in self.order:
            for c in sorted(parent):
                if parent[c] == o:
                    self.depth[c] = self.depth[o] + 1
                    self.order.append(c)
        self.children = {o: [c for c in self.order if parent.get(c) == o] for o in self.order}
        self.groups = [
            [o for o in self.order if low <= self.depth[o] <= high]
            for low, high in ((0, 1), (2, 2), (3, 9))
        ]
        self.groups = [g for g in self.groups if g]
        relays = [o for o in self.order if self.children[o]]
        leaf_groups = [
            i for i, g in enumerate(self.groups) if any(not self.children[o] for o in g)
        ]
        group_of = {o: i for i, g in enumerate(self.groups) for o in g}
        self.lane = {o: i - 1 for i, o in enumerate(relays)}
        for o in self.order:
            if o not in self.lane:
                self.lane[o] = len(relays) - 1 + leaf_groups.index(group_of[o])
        self.lanes = len(relays) - 1 + len(leaf_groups)
        self.sum_lane = {o: i for i, o in enumerate(relays)}
        self.sum_lanes = len(relays)


def chunk_trees(nx, ny):
    return [Tree(nx, ny, KINDS[k], k) for k in range(CHUNKS)]


def signed(v, n):
    return (v + n // 2 - 1) % n - (n // 2 - 1)


def plan(trees, nx, ny, rows, arrivals, urgency, sum_urgency, lead):
    wire, latency, hop = rows * 256 / 46.65e3, 3.2, 0.75
    link, now, steps, pending = {}, 0.0, [], []
    arrived, summed, passed, given = {}, {}, {}, {}

    def sent(p, o):
        dx, dy = signed(o[0] - p[0], nx), signed(o[1] - p[1], ny)
        end = now
        for axis, v, n in ((0, dx, nx), (1, dy, ny)):
            if v:
                for way in (1, -1) if 2 * v == n else (1 if v > 0 else -1,):
                    link[axis, way] = max(link.get((axis, way), 0.0), now) + wire
                    end = max(end, link[axis, way])
        return end + latency + hop * (abs(dx) + abs(dy) - 1)

    def way(p, o):
        dx, dy = signed(o[0] - p[0], nx), signed(o[1] - p[1], ny)
        return (0, 1 if dx > 0 else -1) if dx else (1, 1 if dy > 0 else -1)

    for k in range(len(trees)):
        pending.append(("pass", k, (0, 0)))
        passed[k], given[k] = set(), 0
    finished = 0
    while finished < len(trees):
        ready = {}
        for e in pending:
            kind, k, o = e
            if kind == "pass":
                ready[e] = arrived[k, o] if o != (0, 0) else arrivals[k]
                ways = [way(o, c) for c in trees[k].children[o]]
            elif kind == "sum":
                ready[e] = max([summed[k, c] for c in trees[k].children[o]], default=0.0)
                ways = [way(o, trees[k].parent[o])] if o != (0, 0) else []
            else:
                ready[e] = 0.0
                ways = []
            if ways:
                ready[e] = max(ready[e], min(link.get(w, 0.0) for w in ways) - lead)

        def rank(e):
            kind, k, o = e
            late = -trees[k].depth[o] if kind == "sum" else 0
            first = (sum_urgency if kind == "sum" else urgency)[k]
            return ({"pass": 0, "sum": 0, "finish": 1}.get(kind, 2), first, late, str(o))

        able = [e for e in pending if ready[e] <= now + 1e-9]
        if able:
            e = min(able, key=rank)
        else:
            e = min(pending, key=lambda e: (ready[e], rank(e)))
        pending.remove(e)
        now = max(now, ready[e])
        steps.append(e)
        kind, k, o = e
        tree = trees[k]
        if kind == "pass":
            for c in tree.children[o]:
                arrived[k, c] = sent(o, c)
                pending.append(("pass", k, c))
            now += 0.04
            passed[k].add(o)
            while given[k] < len(tree.groups) and passed[k].issuperset(tree.groups[given[k]]):
                pending.append(("multiply", k, given[k]))
                given[k] += 1
        elif kind == "multiply":
            now += 0.15
            if given[k] == len(tree.groups) and not any(e[:2] == (kind, k) for e in pending):
                pending.append(("finish", k, 0))
        elif kind == "finish":
            now += 0.38
            pending += [("sum", k, c) for c in tree.order if not tree.children[c]]
        else:
            now += 0.05 if tree.children[o] else 0.02
            if o == (0, 0):
                finished += 1
            else:
                p = tree.parent[o]
                summed[k, o] = sent(o, p)
                if all((k, c) in summed for c in tree.children[p]):
                    pending.append(("sum", k, p))
    return steps


def layer_kernel(
    ns,
    nx,
    ny,
    *refs,
):
    sources, (out_ref, *scratch) = refs[:14], refs[14:]
    (
        residual_ref,
        value_ref,
        gate_ref,
        taps_ref,
        conv_bias_ref,
        ln_gain_ref,
        ln_bias_ref,
        out_weight,
        norm_gain_ref,
        ids_ref,
        route_weight_ref,
        expert_gate,
        expert_up,
        expert_down,
    ) = scratch[:14]
    (
        halo,
        gated,
        padded,
        stat,
        gains,
        act,
        mixed,
        picks,
        places,
        route_cols,
        outgoing,
        xbuf,
        acc_gate,
        acc_up,
        acc_sq,
        partial,
        rs_in,
        rs_out,
        ret_out,
        ret_in,
        met,
        load_sem,
        halo_s,
        halo_r,
        stat_s,
        stat_r,
        act_s,
        act_r,
        z_s,
        z_r,
        ag_s,
        ag_r,
        rs_s,
        rs_r,
        rt_s,
        rt_r,
    ) = scratch[14:]
    ntp = nx * ny
    rows, width = residual_ref.shape
    total_width = ntp * width
    slots = places.shape[0]
    cap = slots // ns
    chunks = xbuf.shape[0]
    depth_rows = slots // chunks
    per_side = ns // (2 * chunks)
    taps = taps_ref.shape[0]
    reach = taps // 2
    edge = halo.shape[1]
    s = lax.axis_index("sp")
    t = lax.axis_index("tp")
    ty, tx = t // nx, lax.rem(t, nx)
    trees = chunk_trees(nx, ny)
    ag_base = [sum(tree.lanes for tree in trees[:k]) for k in range(chunks)]
    rs_base = [sum(tree.sum_lanes for tree in trees[:k]) for k in range(chunks)]
    offsets = sorted(trees[0].order, key=lambda o: (abs(signed(o[0], nx)) + abs(signed(o[1], ny)), o))
    number = {o: i for i, o in enumerate(offsets)}

    def tp_at(dx, dy):
        return lax.rem(ty + dy + 2 * ny, ny) * nx + lax.rem(tx + dx + 2 * nx, nx)

    def owner(o):
        return tp_at(-o[0], -o[1])

    def sp_at(d):
        return lax.rem(s + d + 2 * ns, ns)

    def distance(k, jj):
        return k * per_side + jj if jj < per_side else jj - (k + 2) * per_side

    def meet(r):
        if r > 0 and 2 ** (r - 1) < ns // 2:
            pl.semaphore_wait(met.at[r - 1], 2)
        if 2**r < ns // 2:
            for d in (2**r, -(2**r)):
                pl.semaphore_signal(
                    met.at[r], inc=1, device_id=(sp_at(d), t), device_id_type=MESH
                )

    def all_of(ref, sem):
        return pltpu.make_async_copy(ref, ref, sem)

    def send(src, dst, send_sem, recv_sem, device):
        copy = pltpu.make_async_remote_copy(
            src_ref=src,
            dst_ref=dst,
            send_sem=send_sem,
            recv_sem=recv_sem,
            device_id=device,
            device_id_type=MESH,
        )
        copy.start()
        return copy

    with jax.named_scope("signal"):
        barrier = pltpu.get_barrier_semaphore()
        for i in range(1, ntp):
            pl.semaphore_signal(
                barrier, inc=1, device_id=(s, lax.rem(t + i, ntp)), device_id_type=MESH
            )
        for d in (1, -1):
            pl.semaphore_signal(barrier, inc=1, device_id=(sp_at(d), t), device_id_type=MESH)

        loads = {}
        for i in (1, 2, 9, 3, 4, 5, 6, 8, 10, 0, 7, 11, 12, 13):
            source = sources[i].at[0] if i >= 11 else sources[i]
            loads[i] = pltpu.make_async_copy(source, scratch[i], load_sem.at[i])
        for load in loads.values():
            load.start()

    with jax.named_scope("local"):
        loads[1].wait()
        loads[2].wait()
        gated_f = value_ref[...].astype(F32) * jax.nn.sigmoid(gate_ref[...].astype(F32))
        gated[...] = gated_f.astype(BF16)
        padded[edge : edge + rows, :] = gated[...].astype(F32)

    with jax.named_scope("barrier"):
        pl.semaphore_wait(barrier, ntp - 1 + 2)
        meet(0)

    with jax.named_scope("halo"):
        for side, start, d in ((0, rows - edge, 1), (1, 0, -1)):
            send(
                gated.at[pl.ds(start, edge)],
                halo.at[side],
                halo_s.at[0],
                halo_r.at[0],
                (sp_at(d), t),
            )
        far_first = list(reversed(offsets[1:]))
        for i in (5, 6, 8):
            loads[i].wait()
        gains[t] = jnp.concatenate(
            [
                jnp.zeros((2, width), F32),
                1.0 / norm_gain_ref[...],
                ln_gain_ref[...],
                ln_bias_ref[...],
                jnp.zeros((3, width), F32),
            ],
            axis=0,
        )
        for o in far_first:
            send(gains.at[t], gains.at[t], stat_s.at[0], stat_r.at[0], (s, tp_at(*o)))
        meet(1)
        all_of(halo, halo_r.at[0]).wait()
        padded[0:edge, :] = jnp.where(s > 0, halo[0].astype(F32), 0.0)
        padded[edge + rows : edge + rows + edge, :] = jnp.where(
            s < ns - 1, halo[1].astype(F32), 0.0
        )
    with jax.named_scope("conv"):
        for i in (3, 4):
            loads[i].wait()
        tap_values = taps_ref[...].astype(F32)
        conv = jnp.zeros((rows, width), F32) + conv_bias_ref[...]
        for tap in range(taps):
            start = edge - reach + tap
            conv = conv + padded[start : start + rows, :] * tap_values[tap : tap + 1, :]
        conv_t = conv.T
        stat[t, 0:1, :] = jnp.sum(conv_t, axis=0, keepdims=True)
        stat[t, 1:2, :] = jnp.sum(conv_t * conv_t, axis=0, keepdims=True)
        sums_here = stat.at[t, pl.ds(0, 2)]
        for o in far_first:
            send(sums_here, sums_here, stat_s.at[1], stat_r.at[1], (s, tp_at(*o)))
        own_mean = jnp.sum(conv, axis=1, keepdims=True) * (1.0 / width)
        act[0] = (conv - own_mean).astype(BF16)
        half = ntp // 2
        for n, o in enumerate(far_first):
            sem = act_r.at[0 if n + 1 < half else 1]
            send(act.at[0], act.at[number[o]], act_s.at[0], sem, (s, tp_at(*o)))
    with jax.named_scope("route"):
        meet(2)
        for i in (9, 10, 0):
            loads[i].wait()
        expert_of = lax.broadcasted_iota(jnp.int32, (ns, rows), 0)
        chosen = [
            jnp.where(ids_ref[k : k + 1, :] == expert_of, 1.0, 0.0).astype(BF16)
            for k in range(TOPK)
        ]
        earlier = jnp.where(
            lax.broadcasted_iota(jnp.int32, (rows, rows), 0)
            < lax.broadcasted_iota(jnp.int32, (rows, rows), 1),
            1.0,
            0.0,
        ).astype(BF16)
        rank = jnp.dot(chosen[0] + chosen[1], earlier, preferred_element_type=F32).astype(BF16)
        slot = lax.broadcasted_iota(jnp.int32, (slots, ns), 0)
        in_chunk = (slot // cap) & (2 * per_side - 1)
        chunk_of = slot // depth_rows
        away = in_chunk + chunk_of * per_side
        away = jnp.where(in_chunk >= per_side, away - (2 * chunk_of + 2) * per_side, away)
        spread = jnp.where(
            lax.broadcasted_iota(jnp.int32, (slots, ns), 1) == ((s + away + 2 * ns) & (ns - 1)),
            1.0,
            0.0,
        ).astype(BF16)
        rank_at = jnp.dot(spread, rank, preferred_element_type=F32)
        slot_rank = (lax.broadcasted_iota(jnp.int32, (slots, rows), 0) & (cap - 1)).astype(F32)
        hit = rank_at == slot_rank
        both = jnp.zeros((slots, rows), F32)
        for k in range(TOPK):
            here = jnp.dot(spread, chosen[k], preferred_element_type=F32)
            here = jnp.where(hit, here, 0.0)
            picks[k] = here.T.astype(BF16)
            both = both + here
            route_cols[k] = jnp.broadcast_to(route_weight_ref[k : k + 1, :], (width, rows)).T
        places[...] = both.astype(BF16)
    with jax.named_scope("stats"):
        meet(3)
        all_of(gains.at[pl.ds(0, ntp - 1)], stat_r.at[0]).wait()
        all_of(stat.at[pl.ds(0, ntp - 1), pl.ds(0, 2)], stat_r.at[1]).wait()
        totals = jnp.sum(stat[:, 0:2, :], axis=0) * (1.0 / total_width)
        mean = totals[0:1, :]
        spread_inv = lax.rsqrt(totals[1:2, :] - mean * mean + 1e-05)
        lifts = [
            (stat[owner(o), 0:1, :] * (1.0 / width) - mean) * spread_inv for o in offsets
        ]
        lifts.append(spread_inv)
        lifts.append(jnp.zeros((rows - len(lifts), rows), F32))
        columns = jnp.concatenate(lifts, axis=0).T
        inv_col = columns[:, ntp : ntp + 1]
        total = residual_ref[...].astype(F32)
        loads[7].wait()
    with jax.named_scope("act_gather"):
        waiting = [(0, 0)] + far_first
        for n, group in enumerate((waiting[:half], waiting[half:])):
            blocks, tall = [], []
            if n == 1 or half > 1:
                all_of(act.at[pl.ds(0, half - 1 + n)], act_r.at[n]).wait()
            for o in group:
                i = number[o]
                who = owner(o)
                value = act[i].astype(F32) * inv_col + columns[:, i : i + 1]
                value = value * gains[who, 3:4, :] + gains[who, 4:5, :]
                blocks.append(jax.nn.silu(value).astype(BF16))
                tall.append(out_weight[pl.ds(pl.multiple_of(who * width, width), width), :])
            total = total + jnp.dot(
                jnp.concatenate(blocks, axis=1),
                jnp.concatenate(tall, axis=0),
                preferred_element_type=F32,
            )
    with jax.named_scope("project"):
        meet(4)
        mixed[...] = total
        scaled_rows = (total * norm_gain_ref[...]).astype(BF16)

    with jax.named_scope("dispatch"):
        outgoing[...] = jnp.dot(places[...], scaled_rows, preferred_element_type=F32).astype(BF16)
        for k in SEND_ORDER:
            for jj in range(2 * per_side):
                d = distance(k, jj)
                part, flat = pl.ds(jj * cap, cap), pl.ds(k * depth_rows + jj * cap, cap)
                if d == 0:
                    xbuf[k, 0, part, :] = outgoing[flat, :]
                else:
                    send(
                        outgoing.at[flat], xbuf.at[k, 0, part], z_s.at[0], z_r.at[k], (sp_at(d), t)
                    )
        for i in (11, 12, 13):
            loads[i].wait()

    def blocks_of(buffer, k, count):
        return buffer.at[k, pl.ds(0, count)]

    def arriving_leaves(k, index):
        tree = trees[k]
        return [o for o in tree.groups[index] if o != (0, 0) and not tree.children[o]]

    def pass_on(k, o):
        tree = trees[k]
        if o == (0, 0):
            here = cap if distance(k, 0) == 0 else 0
            all_of(xbuf.at[k, 0, pl.ds(0, depth_rows - here)], z_r.at[k]).wait()
        elif tree.children[o]:
            all_of(xbuf.at[k, number[o]], ag_r.at[ag_base[k] + tree.lane[o]]).wait()
        for c in tree.children[o]:
            sem = ag_r.at[ag_base[k] + tree.lane[c]]
            send(
                xbuf.at[k, number[o]],
                xbuf.at[k, number[c]],
                ag_s.at[0],
                sem,
                (s, tp_at(c[0] - o[0], c[1] - o[1])),
            )

    def multiply(k, index):
        group, first = trees[k].groups[index], index == 0
        leaves = arriving_leaves(k, index)
        if leaves:
            sem = ag_r.at[ag_base[k] + trees[k].lane[leaves[0]]]
            all_of(blocks_of(xbuf, k, len(leaves)), sem).wait()
        blocks = [xbuf[k, number[o]] for o in group]
        owners = [owner(o) for o in group]
        wide = jnp.concatenate(blocks, axis=1)
        squares = None if first else acc_sq[k]
        for block, who in zip(blocks, owners):
            plain = block.astype(F32) * gains[who, 2:3, :]
            squares = plain * plain if squares is None else squares + plain * plain
        acc_sq[k] = squares
        for weight, acc in ((expert_gate, acc_gate), (expert_up, acc_up)):
            tall = jnp.concatenate(
                [weight[pl.ds(pl.multiple_of(who * width, width), width), :] for who in owners],
                axis=0,
            )
            product = jnp.dot(wide, tall, preferred_element_type=F32)
            acc[k] = product if first else acc[k] + product

    def finish_rows(k):
        square = jnp.sum(acc_sq[k], axis=1, keepdims=True) * (1.0 / total_width)
        scale = lax.rsqrt(square + 1e-06)
        hidden = (jax.nn.silu(acc_gate[k] * scale) * (acc_up[k] * scale)).astype(BF16)
        for i in range(0, ntp, 2):
            pair = jnp.dot(
                hidden, expert_down[:, i * width : (i + 2) * width], preferred_element_type=F32
            ).astype(BF16)
            partial[k, i] = pair[:, :width]
            partial[k, i + 1] = pair[:, width:]

    def sum_up(k, o):
        who = owner(o)
        tree = trees[k]
        source = partial.at[k, who]
        if tree.children[o]:
            count = len(tree.children[o])
            all_of(blocks_of(rs_in, k, count), rs_r.at[rs_base[k] + tree.sum_lane[o]]).wait()
            value = partial[k, who].astype(F32)
            for c in tree.children[o]:
                value = value + rs_in[k, number[c]].astype(F32)
            if o == (0, 0):
                ret_out[pl.ds(k * depth_rows, depth_rows), :] = value.astype(BF16)
                return
            rs_out[k, number[o]] = value.astype(BF16)
            source = rs_out.at[k, number[o]]
        p = tree.parent[o]
        send(
            source,
            rs_in.at[k, number[o]],
            rs_s.at[0],
            rs_r.at[rs_base[k] + tree.sum_lane[p]],
            (s, tp_at(p[0] - o[0], p[1] - o[1])),
        )

    def give_back(k):
        for jj in range(2 * per_side):
            d = distance(k, jj)
            part = pl.ds(k * depth_rows + jj * cap, cap)
            if d == 0:
                ret_in[part, :] = ret_out[part, :]
            else:
                send(ret_out.at[part], ret_in.at[part], rt_s.at[0], rt_r.at[0], (sp_at(-d), t))

    along = [5.6 * (2 * k + 1) / chunks**2 for k in range(chunks)]
    arrivals, clock = {}, 0.0
    for k in SEND_ORDER:
        clock += along[k]
        arrivals[k] = clock + 1.7 + 0.8 * (8 / chunks) * (k + 1)
    for kind, k, o in plan(trees, nx, ny, depth_rows, arrivals, URGENCY, SUM_URGENCY, LEAD):
        with jax.named_scope(f"{kind}{k}{o}"):
            if kind == "pass":
                pass_on(k, o)
            elif kind == "multiply":
                multiply(k, o)
            elif kind == "finish":
                finish_rows(k)
            else:
                sum_up(k, o)
                if o == (0, 0):
                    give_back(k)
    away_rows = pl.ds(0, slots - cap)
    with jax.named_scope("wait_sends"):
        all_of(halo, halo_s.at[0]).wait()
        all_of(gains.at[pl.ds(0, ntp - 1)], stat_s.at[0]).wait()
        all_of(stat.at[pl.ds(0, ntp - 1), pl.ds(0, 2)], stat_s.at[1]).wait()
        all_of(act.at[pl.ds(0, ntp - 1)], act_s.at[0]).wait()
        all_of(outgoing.at[away_rows], z_s.at[0]).wait()
        all_of(xbuf.at[:, pl.ds(0, ntp - 1)], ag_s.at[0]).wait()
        all_of(rs_in.at[:, pl.ds(0, ntp - 1)], rs_s.at[0]).wait()
    with jax.named_scope("wait_back"):
        all_of(ret_in.at[away_rows], rt_r.at[0]).wait()
    with jax.named_scope("result"):
        answer = ret_in[...]
        result = mixed[...]
        for k in range(TOPK):
            picked = jnp.dot(picks[k], answer, preferred_element_type=F32)
            result = result + picked * route_cols[k]
        out_ref[...] = result.astype(BF16)

    with jax.named_scope("end"):
        all_of(ret_out.at[away_rows], rt_s.at[0]).wait()


def on_device(ns, nx, ny, *args):
    (
        residual,
        glu_value,
        glu_gate,
        conv_weight,
        conv_bias,
        ln_gain,
        ln_bias,
        out_weight,
        norm_gain,
        route_ids,
        route_weight,
        expert_gate,
        expert_up,
        expert_down,
    ) = args
    ntp = nx * ny
    rows, width = residual.shape
    hidden = expert_gate.shape[2]
    capacity = 2 * rows * TOPK // ns
    slots = ns * capacity
    k, rc = CHUNKS, slots // CHUNKS
    edge = 16
    row = lambda v: v.reshape(1, -1)
    vmem = pl.BlockSpec(memory_space=pltpu.VMEM)
    hbm = pl.BlockSpec(memory_space=pltpu.HBM)
    dma = pltpu.SemaphoreType.DMA
    operands = (
        residual,
        glu_value,
        glu_gate,
        conv_weight,
        row(conv_bias),
        row(ln_gain),
        row(ln_bias),
        out_weight,
        row(norm_gain),
        route_ids.T,
        route_weight.T,
        expert_gate,
        expert_up,
        expert_down,
    )
    return pl.pallas_call(
        functools.partial(layer_kernel, ns, nx, ny),
        out_shape=jax.ShapeDtypeStruct(residual.shape, BF16),
        in_specs=[hbm] * 14,
        out_specs=vmem,
        scratch_shapes=[
            *[pltpu.VMEM(a.shape[-2:], a.dtype) for a in operands],
            pltpu.VMEM((2, edge, width), BF16),
            pltpu.VMEM((rows, width), BF16),
            pltpu.VMEM((rows + 2 * edge, width), F32),
            pltpu.VMEM((ntp, 8, width), F32),
            pltpu.VMEM((ntp, 8, width), F32),
            pltpu.VMEM((ntp, rows, width), BF16),
            pltpu.VMEM((rows, width), F32),
            pltpu.VMEM((TOPK, rows, slots), BF16),
            pltpu.VMEM((slots, rows), BF16),
            pltpu.VMEM((TOPK, rows, width), F32),
            pltpu.VMEM((slots, width), BF16),
            pltpu.VMEM((k, ntp, rc, width), BF16),
            pltpu.VMEM((k, rc, hidden), F32),
            pltpu.VMEM((k, rc, hidden), F32),
            pltpu.VMEM((k, rc, width), F32),
            pltpu.VMEM((k, ntp, rc, width), BF16),
            pltpu.VMEM((k, ntp, rc, width), BF16),
            pltpu.VMEM((k, ntp, rc, width), BF16),
            pltpu.VMEM((slots, width), BF16),
            pltpu.VMEM((slots, width), BF16),
            pltpu.SemaphoreType.REGULAR((4,)),
            dma((14,)),
            dma((1,)),
            dma((1,)),
            dma((2,)),
            dma((2,)),
            dma((1,)),
            dma((2,)),
            dma((1,)),
            dma((k,)),
            dma((1,)),
            dma((sum(tree.lanes for tree in chunk_trees(nx, ny)),)),
            dma((1,)),
            dma((sum(tree.sum_lanes for tree in chunk_trees(nx, ny)),)),
            dma((1,)),
            dma((1,)),
        ],
        compiler_params=pltpu.CompilerParams(
            collective_id=0, has_side_effects=True, vmem_limit_bytes=66 * 1000 * 1000
        ),
        name="layer",
    )(*operands)


IN_SPECS = (
    P("sp", "tp"),
    P("sp", "tp"),
    P("sp", "tp"),
    P(None, "tp"),
    P("tp"),
    P("tp"),
    P("tp"),
    P(None, "tp"),
    P("tp"),
    P("sp", None),
    P("sp", None),
    P("sp", None, "tp"),
    P("sp", None, "tp"),
    P("sp", "tp", None),
)


def solution(mesh, nx=NX):
    ns, ntp = mesh.shape["sp"], mesh.shape["tp"]
    return jax.shard_map(
        functools.partial(on_device, ns, nx, ntp // nx),
        mesh=mesh,
        in_specs=IN_SPECS,
        out_specs=P("sp", "tp"),
        check_vma=False,
    )
```
